1024 devices in a mesh: tp: 128 (over z, y), dp: 8 (over x, core).
Axes of the slice: x: 4, y: 4, z: 32, core: 2. Of those that a mesh axis runs over, the one named last changes fastest.
Arguments:
- incoming_token: bfloat16 [256, 4096], P(None, 'dp'), may hold values from -60 to 60
- input_norm_gain: float32 [2, 4096], P(None, 'dp'), may hold values from 0.1 to 1.9
- receptance_weight: bfloat16 [2, 4096, 8192], P(None, 'dp', 'tp'), may hold values from -0.09375 to 0.09375
- key_weight: bfloat16 [2, 4096, 8192], P(None, 'dp', 'tp'), may hold values from -0.09375 to 0.09375
- value_weight: bfloat16 [2, 4096, 8192], P(None, 'dp', 'tp'), may hold values from -0.09375 to 0.09375
- decay_weight: bfloat16 [2, 4096, 8192], P(None, 'dp', 'tp'), may hold values from -0.09375 to 0.09375
- learning_rate_weight: bfloat16 [2, 4096, 8192], P(None, 'dp', 'tp'), may hold values from -0.09375 to 0.09375
- gate_weight: bfloat16 [2, 4096, 8192], P(None, 'dp', 'tp'), may hold values from -0.09375 to 0.09375
- channel_decay_floor: float32 [2, 8192], P(None, 'tp'), may hold values from -5 to 2
- direct_token_weight: float32 [2, 8192], P(None, 'tp'), may hold values from -0.6 to 0.6
- head_norm_gain: float32 [2, 8192], P(None, 'tp'), may hold values from 0.1 to 1.9
- output_weight: bfloat16 [2, 8192, 4096], P(None, 'tp', 'dp'), may hold values from -0.0625 to 0.0625
- incoming_state: float32 [2, 256, 128, 64, 64], P(None, 'dp', 'tp'), may hold values from -6 to 6
Outputs:
- hidden_out: bfloat16 [256, 4096], P(None, 'dp')
- state_out: float32 [2, 256, 128, 64, 64], P(None, 'dp', 'tp')
The draws below stay inside these ranges and needn't reach their ends.
All inputs are finite; a program needn't handle non-finite values.
Results may differ from the reference program's by a relative error of at most 0.0053.
Values may be sent and summed in bfloat16 or wider, within the bound.
A program may use at most 32 MiB of HBM per device.

```python
import jax
import jax.numpy as jnp
from jax import lax

D = 4096
HEADS = 128
HEAD_CHANNELS = 64
MIXER_WIDTH = 8192
BATCH = 256


def draw_incoming_token(key, part):
    key_base = jax.random.fold_in(key, 11)
    key_rows = jax.random.fold_in(key, 12)
    column_rise = jnp.exp(jnp.log(3.0) * jnp.arange(D, dtype=jnp.float32) / (D - 1))
    base_draw = jnp.clip(jax.random.normal(key_base, (BATCH, D), jnp.float32), -4.0, 4.0)
    row_scale = jnp.exp(jax.random.uniform(key_rows, (BATCH, 1), jnp.float32, 0.0, jnp.log(10.0)))
    return (0.5 * base_draw * row_scale * column_rise[None, :]).astype(jnp.bfloat16)


def level_of(key, shape, shards, least, top_value):
    level = 1.0
    for axis_at, blocks in shards:
        steps = jax.random.uniform(jax.random.fold_in(jax.random.fold_in(key, 6), axis_at), (blocks,), jnp.float32, least / len(shards), top_value / len(shards))
        level = level * jnp.repeat(jnp.exp(steps), shape[axis_at] // blocks).reshape((-1,) + (1,) * (len(shape) - 1 - axis_at))
    return level


def gaussian(key, dims, deviation, limit, pieces=(), kind=jnp.bfloat16):
    result = jax.random.normal(key, dims, jnp.float32) * deviation
    if len(pieces) > 0:
        result = level_of(key, dims, pieces, -0.22, 0.18) * result
    return jnp.clip(result, min=-limit, max=limit).astype(kind)


def setup_inputs(seed: int = 0) -> dict:
    arg_keys = jax.random.split(jax.random.key(seed), 14)
    return {
        "incoming_token": draw_incoming_token(jax.random.fold_in(arg_keys[13], 71), 0),
        "input_norm_gain": jnp.clip(1.0 + 0.18 * jax.random.normal(arg_keys[1], (2, D), jnp.float32), 0.1, 1.9),
        "receptance_weight": gaussian(arg_keys[2], (2, D, MIXER_WIDTH), D ** -0.5, 0.09375, ((1, 8), (2, 128))),
        "key_weight": gaussian(arg_keys[3], (2, D, MIXER_WIDTH), D ** -0.5, 0.09375, ((1, 8), (2, 128))),
        "value_weight": gaussian(arg_keys[4], (2, D, MIXER_WIDTH), D ** -0.5, 0.09375, ((1, 8), (2, 128))),
        "decay_weight": gaussian(arg_keys[5], (2, D, MIXER_WIDTH), D ** -0.5, 0.09375, ((1, 8), (2, 128))),
        "learning_rate_weight": gaussian(arg_keys[6], (2, D, MIXER_WIDTH), D ** -0.5, 0.09375, ((1, 8), (2, 128))),
        "gate_weight": gaussian(arg_keys[7], (2, D, MIXER_WIDTH), D ** -0.5, 0.09375, ((1, 8), (2, 128))),
        "channel_decay_floor": jnp.clip(-5.0 + 7.0 * jax.random.uniform(arg_keys[8], (2, MIXER_WIDTH), jnp.float32) ** level_of(arg_keys[8], (2, MIXER_WIDTH), ((1, 128),), -0.2, 0.2), -5.0, 2.0),
        "direct_token_weight": gaussian(arg_keys[9], (2, MIXER_WIDTH), 0.1, 0.6, ((1, 128),), jnp.float32),
        "head_norm_gain": jnp.clip(1.0 + 0.18 * jax.random.normal(arg_keys[10], (2, MIXER_WIDTH), jnp.float32), 0.1, 1.9),
        "output_weight": gaussian(arg_keys[11], (2, MIXER_WIDTH, D), MIXER_WIDTH ** -0.5, 0.0625, ((1, 128), (2, 8))),
        "incoming_state": gaussian(arg_keys[12], (2, BATCH, HEADS, HEAD_CHANNELS, HEAD_CHANNELS), 1.0, 6.0, ((1, 8), (2, 128)), jnp.float32),
    }


def recurrent_mix_heads(projected_output, earlier_state, channel_decay_floor, direct_token_weight, head_norm_gain):
    step_count = projected_output.shape[0]
    local_heads = channel_decay_floor.shape[0] // HEAD_CHANNELS
    sections = projected_output.reshape(step_count, 6, local_heads, HEAD_CHANNELS)
    receptance_rows, keyvec, value_vector, pre_decay, pre_rate, pre_gate = [sections[:, part_index] for part_index in range(6)]
    decay_pre = channel_decay_floor.reshape(local_heads, HEAD_CHANNELS) + pre_decay
    decay_factor = jnp.exp(-jnp.exp(-jax.nn.softplus(-decay_pre) - 0.5))
    learn_rate = jax.nn.sigmoid(pre_rate)
    output_gate_value = jax.nn.sigmoid(pre_gate)
    unit_key = keyvec * lax.rsqrt(lax.optimization_barrier(jnp.sum(keyvec * keyvec, axis=-1, keepdims=True)) + 1e-06)
    rescaled_key = keyvec * learn_rate
    removed = -jnp.einsum('shvk,shk->shv', earlier_state, unit_key, precision=lax.Precision.HIGHEST)
    refreshed_state = earlier_state * decay_factor[:, :, None, :] + removed[..., None] * (unit_key * learn_rate)[:, :, None, :] + value_vector[..., None] * rescaled_key[:, :, None, :]
    readout = jnp.einsum('shvk,shk->shv', refreshed_state, receptance_rows, precision=lax.Precision.HIGHEST)
    group_mean = lax.optimization_barrier(jnp.mean(readout, axis=-1, keepdims=True))
    group_var = lax.optimization_barrier(jnp.mean(jnp.square(readout - group_mean), axis=-1, keepdims=True))
    normalized_input = (readout - group_mean) * lax.rsqrt(group_var + 0.00064) * head_norm_gain.reshape(local_heads, HEAD_CHANNELS)
    direct_token_term = lax.optimization_barrier(jnp.sum(receptance_rows * rescaled_key * direct_token_weight.reshape(local_heads, HEAD_CHANNELS), axis=-1, keepdims=True)) * value_vector
    mixer_output = ((normalized_input + direct_token_term) * output_gate_value).reshape(step_count, local_heads * HEAD_CHANNELS).astype(jnp.bfloat16)
    return (mixer_output, refreshed_state)

def reference(incoming_token, input_norm_gain, receptance_weight, key_weight, value_weight, decay_weight, learning_rate_weight, gate_weight, channel_decay_floor, direct_token_weight, head_norm_gain, output_weight, incoming_state):
    hidden = incoming_token
    new_states = []
    for block_index in range(2):
        hidden_wide = hidden.astype(jnp.float32)
        mean_square = lax.optimization_barrier(jnp.mean(hidden_wide * hidden_wide, axis=-1, keepdims=True))
        scaled_in = (hidden_wide * input_norm_gain[block_index]).astype(jnp.bfloat16)
        matrices = (receptance_weight, key_weight, value_weight, decay_weight, learning_rate_weight, gate_weight)
        projected_output = jnp.concatenate([jnp.dot(scaled_in, matrix[block_index], preferred_element_type=jnp.float32) for matrix in matrices], axis=-1) * lax.rsqrt(mean_square + 1e-06)

        def per_sequence(state_output_pair):
            mixer_output, refreshed_state = recurrent_mix_heads(state_output_pair[0][None], state_output_pair[1][None], channel_decay_floor[block_index], direct_token_weight[block_index], head_norm_gain[block_index])
            return (mixer_output[0], refreshed_state[0])
        mixer_output, refreshed_state = lax.map(per_sequence, (projected_output, incoming_state[block_index]))
        new_states.append(refreshed_state)
        branch = jnp.dot(mixer_output, output_weight[block_index], preferred_element_type=jnp.float32)
        hidden = (hidden_wide + branch).astype(jnp.bfloat16)
    return (hidden, jnp.stack(new_states))
```

```python
import functools

import jax
import jax.numpy as jnp
from jax import lax
from jax.experimental import pallas as pl
from jax.experimental.pallas import tpu as pltpu
from jax.sharding import Mesh
from jax.sharding import PartitionSpec as P

MESH = pl.DeviceIdType.MESH
F32 = jnp.float32
BF16 = jnp.bfloat16
NZ, NY, NX, NC = 32, 4, 4, 2
NDP = NX * NC
D = 4096
HC = 64
SEQ = 32
NT = (((1,), (1,)), ((), ()))
NN = (((1,), (0,)), ((), ()))


def kernel(
    tok_hbm, gain_ref, wr, wk, wv, wd, wa, wg, floor_ref, direct_ref, norm_ref, wo_hbm, st_hbm,
    hid_out, st_out,
    hid, wt, wo, st, st2, psend, precv, osend, oget, ysend, yrecv, zsend, zrecv,
    load_sem, p_ss, p_rs, o_ss, o_rs, y_ss, y_rs, z_ss, z_rs, g_ss, g_rs, h_ss, h_rs, out_sem,
):
    zi, yi = lax.axis_index("z"), lax.axis_index("y")
    xi, ci = lax.axis_index("x"), lax.axis_index("c")
    di = xi * NC + ci

    def dp_peer(k):
        d = lax.rem(di + k, NDP)
        return d, {"x": lax.div(d, NC), "c": lax.rem(d, NC)}

    def y_peer(k):
        p = lax.rem(yi + k, NY)
        return p, {"y": p}

    def z_peer(k):
        p = lax.rem(zi + k, NZ)
        return p, {"z": p}

    def remote(src, dst, ss, rs, dev):
        return pltpu.make_async_remote_copy(
            src_ref=src, dst_ref=dst, send_sem=ss, recv_sem=rs, device_id=dev, device_id_type=MESH
        )

    loads = [pltpu.make_async_copy(tok_hbm, hid.at[0], load_sem.at[0])]
    for l in range(2):
        for p, w in enumerate((wr, wk, wv, wd, wa, wg)):
            loads.append(
                pltpu.make_async_copy(w.at[l], wt.at[l, pl.ds(64 * p, 64)], load_sem.at[1 + 6 * l + p])
            )
    state_loads = [pltpu.make_async_copy(st_hbm.at[l], st.at[l], load_sem.at[13 + l]) for l in range(2)]
    wo_load = pltpu.make_async_copy(wo_hbm, wo, load_sem.at[15])
    for cp in loads[:7]:
        cp.start()
    state_loads[0].start()
    wo_load.start()
    for cp in loads[7:]:
        cp.start()
    state_loads[1].start()

    barrier = pltpu.get_barrier_semaphore()

    def greet_z(k, _):
        pl.semaphore_signal(barrier, inc=1, device_id=z_peer(k)[1], device_id_type=MESH)
        return 0

    lax.fori_loop(1, NZ, greet_z, 0)
    for k in range(1, NDP):
        pl.semaphore_signal(barrier, inc=1, device_id=dp_peer(k)[1], device_id_type=MESH)
    for k in range(1, NY):
        pl.semaphore_signal(barrier, inc=1, device_id=y_peer(k)[1], device_id_type=MESH)

    for l in range(2):
        if l == 0:
            loads[0].wait()
        for cp in loads[1 + 6 * l : 7 + 6 * l]:
            cp.wait()
        hv = hid[l].astype(F32).reshape(NZ, 4, 8, 128)
        sq = None
        xs = []
        for cg in range(4):
            part = hv[:, cg].reshape(256, 128)
            sq = part * part if sq is None else sq + part * part
            xs.append((part * gain_ref[l : l + 1, 128 * cg : 128 * cg + 128]).astype(BF16))
        sq = jnp.sum(sq, axis=1, keepdims=True)
        high = sq.astype(BF16).astype(F32)
        low = sq - high
        lane = lax.broadcasted_iota(jnp.int32, (256, 128), 1)
        tail = jnp.where(lane == 0, high, jnp.where(lane == 1, low, 0.0)).astype(BF16)
        proj = lax.dot_general(
            jnp.concatenate(xs, axis=1), wt[l], NT, preferred_element_type=F32
        ).astype(BF16)
        psend[l, :, :, 0:384] = proj.reshape(NDP, SEQ, 384)
        psend[l, :, :, 384:512] = tail.reshape(NDP, SEQ, 128)
        if l == 0:
            pl.semaphore_wait(barrier, (NZ - 1) + (NDP - 1) + (NY - 1))
        for k in range(1, NDP):
            d, dev = dp_peer(k)
            remote(psend.at[l, d], precv.at[l, di], p_ss.at[l], p_rs.at[l], dev).start()
        total = psend[l, di].astype(F32)
        if l == 0:
            state_loads[0].wait()
        else:
            state_loads[1].wait()
        remote(
            psend.at[l, pl.ds(0, NDP - 1)], precv.at[l, pl.ds(0, NDP - 1)], p_ss.at[l], p_rs.at[l], {"y": lax.rem(yi + 1, NY)}
        ).wait_recv()
        for k in range(1, NDP):
            total = total + precv[l, lax.rem(di + k, NDP)].astype(F32)
        squares = total[:, 384:385] + total[:, 385:386]
        total = total[:, 0:384] * lax.rsqrt(squares * (1.0 / D) + 1e-6)
        r, k_, v, pd, pa, pg = [total[:, 64 * p : 64 * p + 64] for p in range(6)]
        decay = jnp.exp(-0.6065306597126334 * jax.nn.sigmoid(floor_ref[l : l + 1, :] + pd))
        rate = jax.nn.sigmoid(pa)
        gate = jax.nn.sigmoid(pg)
        u = k_ * lax.rsqrt(jnp.sum(k_ * k_, axis=1, keepdims=True) + 1e-6)
        kr = k_ * rate
        ur = u * rate
        dr = decay * r
        row16 = lax.broadcasted_iota(jnp.int32, (16, 64), 0) % 8
        cs, ys = [], []
        for q in range(4):
            rows = slice(8 * q, 8 * q + 8)
            left = jnp.concatenate([u[rows], dr[rows]], axis=0).astype(BF16)
            blk = st[l, rows].reshape(512, 64).astype(BF16)
            res = lax.dot_general(left, blk, NT, preferred_element_type=F32)
            acc = jnp.zeros((16, 64), F32)
            for t in range(8):
                acc = jnp.where(row16 == t, res[:, 64 * t : 64 * t + 64], acc)
            cs.append(acc[0:8])
            ys.append(acc[8:16])
        c = -jnp.concatenate(cs, axis=0)
        y = (
            jnp.concatenate(ys, axis=0)
            + c * jnp.sum(ur * r, axis=1, keepdims=True)
            + v * jnp.sum(kr * r, axis=1, keepdims=True)
        )
        y = y - jnp.mean(y, axis=1, keepdims=True)
        var = jnp.mean(y * y, axis=1, keepdims=True)
        o = y * lax.rsqrt(var + 0.00064) * norm_ref[l : l + 1, :]
        o = o + jnp.sum(r * kr * direct_ref[l : l + 1, :], axis=1, keepdims=True) * v
        o = o * gate
        osend[l] = jnp.concatenate([o, jnp.zeros_like(o)], axis=1).astype(BF16)
        for k in range(1, NDP):
            _, dev = dp_peer(k)
            remote(osend.at[l], oget.at[l, di], o_ss.at[l], o_rs.at[l], dev).start()
        oget[l, di] = osend[l]
        ct = c.T
        vt = v.T

        def update(lo, hi):
            for s in range(lo, hi):
                st2[l, s] = (
                    st[l, s] * decay[s : s + 1, :]
                    + ct[:, s : s + 1] * ur[s : s + 1, :]
                    + vt[:, s : s + 1] * kr[s : s + 1, :]
                )

        if l == 0:
            wo_load.wait()
        remote(
            oget.at[l, pl.ds(0, NDP - 1)], oget.at[l, pl.ds(0, NDP - 1)], o_ss.at[l], o_rs.at[l], {"y": lax.rem(yi + 1, NY)}
        ).wait_recv()
        for k in (2, 1, 3, 0):
            p, dev = y_peer(k)
            rows = oget[l, pl.ds(2 * p, 2)].reshape(64, 128)[:, 0:64]
            share = lax.dot_general(rows, wo[l], NN, preferred_element_type=F32).astype(BF16)
            for rg in range(8):
                for cg in range(4):
                    ysend[l, p, rg * 4 + cg] = share[8 * rg : 8 * rg + 8, 128 * cg : 128 * cg + 128]
            if k:
                remote(ysend.at[l, p], yrecv.at[l, k - 1], y_ss.at[l], y_rs.at[l], dev).start()
        remote(
            yrecv.at[l, pl.ds(0, 3)], yrecv.at[l, pl.ds(0, 3)], y_ss.at[l], y_rs.at[l], {"y": lax.rem(yi + 1, NY)}
        ).wait_recv()
        summed = ysend[l, yi].astype(F32)
        for k in range(3):
            summed = summed + yrecv[l, k].astype(F32)
        zsend[l] = summed.astype(BF16)

        def z_scatter(k, _):
            far = jnp.where(k % 2 == 0, NZ // 2 + k // 2, NZ // 2 - (k + 1) // 2)
            p, dev = z_peer(far)
            remote(zsend.at[l, p], zrecv.at[l, zi], z_ss.at[l], z_rs.at[l], dev).start()
            return 0

        lax.fori_loop(0, NZ - 1, z_scatter, 0)
        zrecv[l, zi] = zsend[l, zi]
        update(0, SEQ)
        state_store = pltpu.make_async_copy(st2.at[l], st_out.at[l], out_sem.at[l])
        state_store.start()
        remote(
            zrecv.at[l, pl.ds(0, NZ - 1)], zrecv.at[l, pl.ds(0, NZ - 1)], z_ss.at[l], z_rs.at[l], {"z": lax.rem(zi + 1, NZ)}
        ).wait_recv()
        mine = jnp.sum(zrecv[l].astype(F32), axis=0) + hid[l, yi, zi].astype(F32)
        hid[l + 1, yi, zi] = mine.astype(BF16)

        def z_gather(k, _):
            far = jnp.where(k % 2 == 0, NZ // 2 + k // 2, NZ // 2 - (k + 1) // 2)
            _, dev = z_peer(far)
            own = hid.at[l + 1, yi, zi]
            remote(own, own, g_ss.at[l], g_rs.at[l], dev).start()
            return 0

        lax.fori_loop(0, NZ - 1, z_gather, 0)
        some = hid.at[l + 1, yi, pl.ds(0, NZ - 1)]
        remote(some, some, g_ss.at[l], g_rs.at[l], {"z": lax.rem(zi + 1, NZ)}).wait_recv()
        for k in (2, 1, 3):
            _, dev = y_peer(k)
            own = hid.at[l + 1, yi]
            remote(own, own, h_ss.at[l], h_rs.at[l], dev).start()
        three = hid.at[l + 1, pl.ds(0, 3)]
        remote(three, three, h_ss.at[l], h_rs.at[l], {"y": lax.rem(yi + 1, NY)}).wait_recv()

    hid_store = pltpu.make_async_copy(hid.at[2], hid_out, out_sem.at[2])
    hid_store.start()
    for l in range(2):
        near = {"y": lax.rem(yi + 1, NY)}
        for buf, count, ss, rs in (
            (psend.at[l, pl.ds(0, NDP - 1)], None, p_ss, p_rs),
            (oget.at[l, pl.ds(0, NDP - 1)], None, o_ss, o_rs),
            (yrecv.at[l, pl.ds(0, 3)], None, y_ss, y_rs),
            (zsend.at[l, pl.ds(0, NZ - 1)], None, z_ss, z_rs),
            (zsend.at[l, pl.ds(0, NZ - 1)], None, g_ss, g_rs),
            (yrecv.at[l, pl.ds(0, 3)], None, h_ss, h_rs),
        ):
            remote(buf, buf, ss.at[l], rs.at[l], near).wait_send()
        pltpu.make_async_copy(st2.at[l], st_out.at[l], out_sem.at[l]).wait()
    hid_store.wait()


def per_device(
    incoming_token, input_norm_gain, receptance_weight, key_weight, value_weight, decay_weight,
    learning_rate_weight, gate_weight, channel_decay_floor, direct_token_weight, head_norm_gain,
    output_weight, incoming_state,
):
    tiles = incoming_token.reshape(NZ, 8, 4, 128).transpose(0, 2, 1, 3).reshape(NY, NZ, 8, 128)
    weights = [
        jnp.swapaxes(w, 1, 2)
        for w in (
            receptance_weight, key_weight, value_weight, decay_weight, learning_rate_weight, gate_weight,
        )
    ]
    state = incoming_state.reshape(2, SEQ, HC, HC)
    anywhere = pl.BlockSpec(memory_space=pl.ANY)
    vmem = pl.BlockSpec(memory_space=pltpu.VMEM)
    dma = pltpu.SemaphoreType.DMA
    hidden, new_state = pl.pallas_call(
        kernel,
        out_shape=(
            jax.ShapeDtypeStruct((NY, NZ, 8, 128), BF16),
            jax.ShapeDtypeStruct((2, SEQ, HC, HC), F32),
        ),
        in_specs=[anywhere, vmem] + [anywhere] * 6 + [vmem] * 3 + [anywhere] * 2,
        out_specs=(anywhere, anywhere),
        scratch_shapes=[
            pltpu.VMEM((3, NY, NZ, 8, 128), BF16),
            pltpu.VMEM((2, 384, 512), BF16),
            pltpu.VMEM((2, HC, 512), BF16),
            pltpu.VMEM((2, SEQ, HC, HC), F32),
            pltpu.VMEM((2, SEQ, HC, HC), F32),
            pltpu.VMEM((2, NDP, SEQ, 512), BF16),
            pltpu.VMEM((2, NDP, SEQ, 512), BF16),
            pltpu.VMEM((2, SEQ, 128), BF16),
            pltpu.VMEM((2, NDP, SEQ, 128), BF16),
            pltpu.VMEM((2, NY, NZ, 8, 128), BF16),
            pltpu.VMEM((2, 3, NZ, 8, 128), BF16),
            pltpu.VMEM((2, NZ, 8, 128), BF16),
            pltpu.VMEM((2, NZ, 8, 128), BF16),
            dma((16,)),
            *[dma((2,)) for _ in range(12)],
            dma((3,)),
        ],
        compiler_params=pltpu.CompilerParams(
            collective_id=0, has_side_effects=True, vmem_limit_bytes=48 * 1024 * 1024
        ),
        name="decode_step",
    )(
        tiles, input_norm_gain, *weights, channel_decay_floor, direct_token_weight, head_norm_gain,
        output_weight, state,
    )
    hidden = hidden.reshape(NZ, 4, 8, 128).transpose(0, 2, 1, 3).reshape(256, 512)
    return (hidden, new_state.reshape(2, SEQ, 1, HC, HC))


def solution(mesh):
    finer = Mesh(mesh.devices.reshape(NZ, NY, NX, NC), ("z", "y", "x", "c"))
    tp, dp = ("z", "y"), ("x", "c")
    w = P(None, dp, tp)
    return jax.shard_map(
        per_device,
        mesh=finer,
        in_specs=(
            P(None, dp), P(None, dp), w, w, w, w, w, w, P(None, tp), P(None, tp), P(None, tp),
            P(None, tp, dp), P(None, dp, tp, None, None),
        ),
        out_specs=(P(None, dp), P(None, dp, tp, None, None)),
        check_vma=False,
    )
```

```python
import functools

import jax
import jax.numpy as jnp
from jax import lax
from jax.experimental import pallas as pl
from jax.experimental.pallas import tpu as pltpu
from jax.sharding import Mesh
from jax.sharding import PartitionSpec as P

MESH = pl.DeviceIdType.MESH
F32 = jnp.float32
BF16 = jnp.bfloat16
NZ, NY, NX, NC = 32, 4, 4, 2
NDP = NX * NC
D = 4096
HC = 64
SEQ = 32
NT = (((1,), (1,)), ((), ()))
NN = (((1,), (0,)), ((), ()))
GROUPS = ((0, 7), (7, 15), (15, 31))


def kernel(
    tok_hbm, gain_hbm, wr, wk, wv, wd, wa, wg, floor_hbm, direct_hbm, norm_hbm, wo_hbm, st_hbm,
    hid_out, st_out,
    hid, gain_ref, floor_ref, direct_ref, norm_ref, wt, wo, st, psend, precv, osend, oget, ysend, yrecv, zsend, zrecv,
    load_sem, p_ss, p_rs, o_ss, o_rs, y_ss, y_rs, z_ss, z_rs, g_ss, g_rs, h_ss, h_rs, within8, within16,
):
    zi, yi = lax.axis_index("z"), lax.axis_index("y")
    xi, ci = lax.axis_index("x"), lax.axis_index("c")
    di = xi * NC + ci

    def dp_peer(k):
        d = lax.rem(di + k, NDP)
        return d, {"x": lax.div(d, NC), "c": lax.rem(d, NC)}

    def y_peer(k):
        p = lax.rem(yi + k, NY)
        return p, {"y": p}

    def z_peer(k):
        p = lax.rem(zi + k, NZ)
        return p, {"z": p}

    def remote(src, dst, ss, rs, dev):
        return pltpu.make_async_remote_copy(
            src_ref=src, dst_ref=dst, send_sem=ss, recv_sem=rs, device_id=dev, device_id_type=MESH
        )

    def far_first(k):
        return jnp.where(k % 2 == 0, NZ // 2 + k // 2, NZ // 2 - (k + 1) // 2)

    def y_copy(l, k, h):
        p, dev = y_peer(k)
        part = pl.ds(16 * h, 16)
        return remote(ysend.at[l, p, part], yrecv.at[l, k - 1, part], y_ss.at[l], y_rs.at[l, h], dev)

    loads = [pltpu.make_async_copy(tok_hbm, hid.at[0], load_sem.at[0])]
    for l in range(2):
        for p, w in enumerate((wr, wk, wv, wd, wa, wg)):
            loads.append(
                pltpu.make_async_copy(w.at[l], wt.at[l, pl.ds(64 * p, 64)], load_sem.at[1 + 6 * l + p])
            )
    state_loads = [pltpu.make_async_copy(st_hbm.at[l], st.at[l], load_sem.at[13 + l]) for l in range(2)]
    wo_load = pltpu.make_async_copy(wo_hbm, wo, load_sem.at[15])
    smalls = [
        pltpu.make_async_copy(a, b, load_sem.at[16 + i])
        for i, (a, b) in enumerate(
            ((gain_hbm, gain_ref), (floor_hbm, floor_ref), (direct_hbm, direct_ref), (norm_hbm, norm_ref))
        )
    ]
    loads[0].start()
    for cp in smalls:
        cp.start()
    for cp in loads[1:7]:
        cp.start()
    state_loads[0].start()
    wo_load.start()
    for cp in loads[7:]:
        cp.start()
    state_loads[1].start()

    barrier = pltpu.get_barrier_semaphore()

    for k in (1, 2, 3, 4, NZ - 4, NZ - 3, NZ - 2, NZ - 1):
        pl.semaphore_signal(barrier, inc=1, device_id=z_peer(k)[1], device_id_type=MESH)
    for k in range(1, NDP):
        pl.semaphore_signal(barrier, inc=1, device_id=dp_peer(k)[1], device_id_type=MESH)
    for k in range(1, NY):
        pl.semaphore_signal(barrier, inc=1, device_id=y_peer(k)[1], device_id_type=MESH)

    for l in range(2):
        if l == 0:
            loads[0].wait()
            for cp in smalls:
                cp.wait()
        for cp in loads[1 + 6 * l : 7 + 6 * l]:
            cp.wait()
        hv = hid[l].astype(F32).reshape(NZ, 4, 8, 128)
        sq = None
        xs = []
        for cg in range(4):
            part = hv[:, cg].reshape(256, 128)
            sq = part * part if sq is None else sq + part * part
            xs.append((part * gain_ref[l : l + 1, 128 * cg : 128 * cg + 128]).astype(BF16))
        sq = jnp.sum(sq, axis=1, keepdims=True)
        high = sq.astype(BF16).astype(F32)
        low = sq - high
        lane = lax.broadcasted_iota(jnp.int32, (256, 128), 1)
        tail = jnp.where(lane == 0, high, jnp.where(lane == 1, low, 0.0)).astype(BF16)
        proj = lax.dot_general(
            jnp.concatenate(xs, axis=1), wt[l], NT, preferred_element_type=F32
        ).astype(BF16)
        psend[l, :, :, 0:384] = proj.reshape(NDP, SEQ, 384)
        psend[l, :, :, 384:512] = tail.reshape(NDP, SEQ, 128)
        if l == 0:
            with jax.named_scope("w_bar"):
                pl.semaphore_wait(barrier, 8 + (NDP - 1) + (NY - 1))
            for k in (4, NZ - 4):
                pl.semaphore_signal(within8, inc=1, device_id=z_peer(k)[1], device_id_type=MESH)
        for k in (4, 3, 5, 2, 6, 1, 7):
            d, dev = dp_peer(k)
            remote(psend.at[l, d], precv.at[l, di], p_ss.at[l], p_rs.at[l], dev).start()
        total = psend[l, di].astype(F32)
        if l == 0:
            with jax.named_scope("w_st"):
                state_loads[0].wait()
        else:
            with jax.named_scope("w_st"):
                state_loads[1].wait()
        with jax.named_scope("w_p"):
            remote(
                psend.at[l, pl.ds(0, NDP - 1)], precv.at[l, pl.ds(0, NDP - 1)], p_ss.at[l], p_rs.at[l], {"y": lax.rem(yi + 1, NY)}
            ).wait_recv()
        if l == 0:
            pl.semaphore_wait(within8, 2)
            for k in (8, NZ - 8):
                pl.semaphore_signal(within16, inc=1, device_id=z_peer(k)[1], device_id_type=MESH)
        for k in range(1, NDP):
            total = total + precv[l, lax.rem(di + k, NDP)].astype(F32)
        squares = total[:, 384:385] + total[:, 385:386]
        total = total[:, 0:384] * lax.rsqrt(squares * (1.0 / D) + 1e-6)
        r, k_, v, pd, pa, pg = [total[:, 64 * p : 64 * p + 64] for p in range(6)]
        decay = jnp.exp(-0.6065306597126334 * jax.nn.sigmoid(floor_ref[l : l + 1, :] + pd))
        rate = jax.nn.sigmoid(pa)
        gate = jax.nn.sigmoid(pg)
        u = k_ * lax.rsqrt(jnp.sum(k_ * k_, axis=1, keepdims=True) + 1e-6)
        kr = k_ * rate
        ur = u * rate
        dr = decay * r
        row16 = lax.broadcasted_iota(jnp.int32, (16, 64), 0) % 8
        cs, ys = [], []
        for q in range(4):
            rows = slice(8 * q, 8 * q + 8)
            left = jnp.concatenate([u[rows], dr[rows]], axis=0).astype(BF16)
            blk = st[l, rows].reshape(512, 64).astype(BF16)
            res = lax.dot_general(left, blk, NT, preferred_element_type=F32)
            acc = jnp.zeros((16, 64), F32)
            for t in range(8):
                acc = jnp.where(row16 == t, res[:, 64 * t : 64 * t + 64], acc)
            cs.append(acc[0:8])
            ys.append(acc[8:16])
        c = -jnp.concatenate(cs, axis=0)
        y = (
            jnp.concatenate(ys, axis=0)
            + c * jnp.sum(ur * r, axis=1, keepdims=True)
            + v * jnp.sum(kr * r, axis=1, keepdims=True)
        )
        y = y - jnp.mean(y, axis=1, keepdims=True)
        var = jnp.mean(y * y, axis=1, keepdims=True)
        o = y * lax.rsqrt(var + 0.00064) * norm_ref[l : l + 1, :]
        o = o + jnp.sum(r * kr * direct_ref[l : l + 1, :], axis=1, keepdims=True) * v
        o = o * gate
        osend[l] = jnp.concatenate([o, jnp.zeros_like(o)], axis=1).astype(BF16)
        for k in (4, 3, 5, 2, 6, 1, 7):
            _, dev = dp_peer(k)
            remote(osend.at[l], oget.at[l, di], o_ss.at[l], o_rs.at[l], dev).start()
        oget[l, di] = osend[l]
        ct = c.T
        vt = v.T

        def update(lo, hi):
            for s in range(lo, hi):
                st_out[l, s] = (
                    st[l, s] * decay[s : s + 1, :]
                    + ct[:, s : s + 1] * ur[s : s + 1, :]
                    + vt[:, s : s + 1] * kr[s : s + 1, :]
                )

        if l == 0:
            wo_load.wait()
        with jax.named_scope("w_o"):
            remote(
                oget.at[l, pl.ds(0, NDP - 1)], oget.at[l, pl.ds(0, NDP - 1)], o_ss.at[l], o_rs.at[l], {"y": lax.rem(yi + 1, NY)}
            ).wait_recv()
        for k in (2, 1, 3, 0):
            p, dev = y_peer(k)
            rows = oget[l, pl.ds(2 * p, 2)].reshape(64, 128)[:, 0:64]
            share = lax.dot_general(rows, wo[l], NN, preferred_element_type=F32).astype(BF16)
            for rg in range(8):
                for cg in range(4):
                    j = lax.rem(rg * 4 + cg + (NZ - 8) + NZ - zi, NZ)
                    ysend[l, p, j] = share[8 * rg : 8 * rg + 8, 128 * cg : 128 * cg + 128]
            if k:
                y_copy(l, k, 0).start()
        for k in (2, 1, 3):
            y_copy(l, k, 1).start()
        if l == 0:
            with jax.named_scope("w_16"):
                pl.semaphore_wait(within16, 2)
        for h in range(2):
            part = pl.ds(16 * h, 16)
            with jax.named_scope("w_y"):
                some = yrecv.at[l, pl.ds(0, 3), part]
                remote(some, some, y_ss.at[l], y_rs.at[l, h], y_peer(1)[1]).wait_recv()
            summed = ysend[l, yi, part].astype(F32)
            for k in range(3):
                summed = summed + yrecv[l, k, part].astype(F32)
            zsend[l, part] = summed.astype(BF16)

            def z_scatter(k, _):
                off = far_first(k)
                _, dev = z_peer(off)
                src = zsend.at[l, lax.rem(off + (NZ - 8), NZ)]
                remote(src, zrecv.at[l, zi], z_ss.at[l], z_rs.at[l], dev).start()
                return 0

            with jax.named_scope("zsend"):
                lax.fori_loop(16 * h, 16 + 15 * h, z_scatter, 0)
        zrecv[l, zi] = zsend[l, NZ - 8]
        with jax.named_scope("upd"):
            update(0, SEQ)
        with jax.named_scope("w_z"):
            some = zrecv.at[l, pl.ds(0, NZ - 1)]
            remote(some, some, z_ss.at[l], z_rs.at[l], z_peer(1)[1]).wait_recv()
        mine = jnp.sum(zrecv[l].astype(F32), axis=0) + hid[l, yi, zi].astype(F32)
        hid[l + 1, yi, zi] = mine.astype(BF16)

        own = hid.at[l + 1, yi, zi]
        for g, (lo, hi) in enumerate(GROUPS):

            def z_gather(k, _):
                _, dev = z_peer(far_first(k))
                remote(own, own, g_ss.at[l], g_rs.at[l, g], dev).start()
                return 0

            with jax.named_scope("zsend"):
                lax.fori_loop(lo, hi, z_gather, 0)

        def forward(chunk):
            for k in (2, 1, 3):
                remote(chunk, chunk, h_ss.at[l], h_rs.at[l], y_peer(k)[1]).start()

        forward(own)
        for g in range(len(GROUPS) - 1, -1, -1):
            lo, hi = GROUPS[g]
            with jax.named_scope("w_g"):
                some = zsend.at[l, pl.ds(0, hi - lo)]
                remote(some, some, g_ss.at[l], g_rs.at[l, g], z_peer(1)[1]).wait_recv()

            def onward(k, _):
                forward(hid.at[l + 1, yi, z_peer(far_first(k))[0]])
                return 0

            with jax.named_scope("fwd"):
                lax.fori_loop(lo, hi, onward, 0)
        three = hid.at[l + 1, pl.ds(0, 3)]
        with jax.named_scope("w_h"):
            remote(three, three, h_ss.at[l], h_rs.at[l], {"y": lax.rem(yi + 1, NY)}).wait_recv()

    hid_out[...] = hid[2]
    for l in range(2):
        near = {"y": lax.rem(yi + 1, NY)}
        for buf, ss in (
            (psend.at[l, pl.ds(0, NDP - 1)], p_ss),
            (oget.at[l, pl.ds(0, NDP - 1)], o_ss),
            (yrecv.at[l, pl.ds(0, 3)], y_ss),
            (zsend.at[l, pl.ds(0, NZ - 1)], z_ss),
            (zsend.at[l, pl.ds(0, NZ - 1)], g_ss),
            (yrecv.at[l, pl.ds(0, 3)], h_ss),
        ):
            remote(buf, buf, ss.at[l], p_rs.at[l], near).wait_send()


def per_device(
    incoming_token, input_norm_gain, receptance_weight, key_weight, value_weight, decay_weight,
    learning_rate_weight, gate_weight, channel_decay_floor, direct_token_weight, head_norm_gain,
    output_weight, incoming_state,
):
    tiles = incoming_token.reshape(NZ, 8, 4, 128).transpose(0, 2, 1, 3).reshape(NY, NZ, 8, 128)
    weights = [
        jnp.swapaxes(w, 1, 2)
        for w in (
            receptance_weight, key_weight, value_weight, decay_weight, learning_rate_weight, gate_weight,
        )
    ]
    state = incoming_state.reshape(2, SEQ, HC, HC)
    anywhere = pl.BlockSpec(memory_space=pl.ANY)
    vmem = pl.BlockSpec(memory_space=pltpu.VMEM)
    dma = pltpu.SemaphoreType.DMA
    hidden, new_state = pl.pallas_call(
        kernel,
        out_shape=(
            pltpu.VMEM((NY, NZ, 8, 128), BF16),
            pltpu.VMEM((2, SEQ, HC, HC), F32),
        ),
        in_specs=[anywhere] * 13,
        out_specs=(vmem, vmem),
        scratch_shapes=[
            pltpu.VMEM((3, NY, NZ, 8, 128), BF16),
            pltpu.VMEM((2, 512), F32),
            *[pltpu.VMEM((2, HC), F32) for _ in range(3)],
            pltpu.VMEM((2, 384, 512), BF16),
            pltpu.VMEM((2, HC, 512), BF16),
            pltpu.VMEM((2, SEQ, HC, HC), F32),
            pltpu.VMEM((2, NDP, SEQ, 512), BF16),
            pltpu.VMEM((2, NDP, SEQ, 512), BF16),
            pltpu.VMEM((2, SEQ, 128), BF16),
            pltpu.VMEM((2, NDP, SEQ, 128), BF16),
            pltpu.VMEM((2, NY, NZ, 8, 128), BF16),
            pltpu.VMEM((2, 3, NZ, 8, 128), BF16),
            pltpu.VMEM((2, NZ, 8, 128), BF16),
            pltpu.VMEM((2, NZ, 8, 128), BF16),
            dma((20,)),
            *[dma((2,)) for _ in range(5)],
            dma((2, 2)),
            *[dma((2,)) for _ in range(3)],
            dma((2, len(GROUPS))),
            *[dma((2,)) for _ in range(2)],
            pltpu.SemaphoreType.REGULAR,
            pltpu.SemaphoreType.REGULAR,
        ],
        compiler_params=pltpu.CompilerParams(
            collective_id=0, has_side_effects=True, vmem_limit_bytes=60 * 1024 * 1024
        ),
        name="decode_step",
    )(
        tiles, input_norm_gain, *weights, channel_decay_floor, direct_token_weight, head_norm_gain,
        output_weight, state,
    )
    hidden = hidden.reshape(NZ, 4, 8, 128).transpose(0, 2, 1, 3).reshape(256, 512)
    return (hidden, new_state.reshape(2, SEQ, 1, HC, HC))


def solution(mesh):
    finer = Mesh(mesh.devices.reshape(NZ, NY, NX, NC), ("z", "y", "x", "c"))
    tp, dp = ("z", "y"), ("x", "c")
    w = P(None, dp, tp)
    return jax.shard_map(
        per_device,
        mesh=finer,
        in_specs=(
            P(None, dp), P(None, dp), w, w, w, w, w, w, P(None, tp), P(None, tp), P(None, tp),
            P(None, tp, dp), P(None, dp, tp, None, None),
        ),
        out_specs=(P(None, dp), P(None, dp, tp, None, None)),
        check_vma=False,
    )
```

```python
import functools

import jax
import jax.numpy as jnp
from jax import lax
from jax.experimental import pallas as pl
from jax.experimental.pallas import tpu as pltpu
from jax.sharding import Mesh
from jax.sharding import PartitionSpec as P

MESH = pl.DeviceIdType.MESH
F32 = jnp.float32
BF16 = jnp.bfloat16
NZ, NY, NX, NC = 32, 4, 4, 2
NDP = NX * NC
D = 4096
HC = 64
SEQ = 32
NT = (((1,), (1,)), ((), ()))
NN = (((1,), (0,)), ((), ()))
GROUPS = ((0, 3), (3, 7), (7, 11), (11, 15))
DIRECT = 0


def kernel(
    tok_hbm, gain_hbm, wr, wk, wv, wd, wa, wg, floor_hbm, direct_hbm, norm_hbm, wo_hbm, st_hbm,
    hid_out, st_out,
    hid, gain_ref, floor_ref, direct_ref, norm_ref, wt, wo, st, stb, tsend, trecv, psend, precv, osend, oget, zsend, zrecv,
    load_sem, t_ss, t_rs, p_ss, p_rs, o_ss, o_rs, w_ss, w_rs, z_ss, z_rs, g_ss, g_rs, h_ss, h_rs, within8, within16,
):
    zi, yi = lax.axis_index("z"), lax.axis_index("y")
    xi, ci = lax.axis_index("x"), lax.axis_index("c")
    di = xi * NC + ci

    def dp_peer(k):
        d = lax.rem(di + k, NDP)
        return d, {"x": lax.div(d, NC), "c": lax.rem(d, NC)}

    def y_peer(k):
        p = lax.rem(yi + k, NY)
        return p, {"y": p}

    def z_peer(k):
        p = lax.rem(zi + k, NZ)
        return p, {"z": p}

    def remote(src, dst, ss, rs, dev):
        return pltpu.make_async_remote_copy(
            src_ref=src, dst_ref=dst, send_sem=ss, recv_sem=rs, device_id=dev, device_id_type=MESH
        )

    def far_first(k):
        return jnp.where(k % 2 == 0, NZ // 2 + k // 2, NZ // 2 - (k + 1) // 2)

    def near_off(k):
        return jnp.where(k % 2 == 0, NZ - 8 + k // 2, 8 - (k + 1) // 2)

    def o_count(l, wait):
        @pl.when(yi != xi)
        def _():
            wait(oget.at[l])

        @pl.when(yi == xi)
        def _():
            wait(oget.at[l, pl.ds(0, NDP - 1)])

    order = []
    for q in range(16):
        apart = lax.rem(q + NZ - zi, 16)
        order.append(jnp.where(apart < 8, 2 * apart, 31 - 2 * apart))

    barrier = pltpu.get_barrier_semaphore()

    for k in (1, 2, 3, 4, NZ - 4, NZ - 3, NZ - 2, NZ - 1):
        pl.semaphore_signal(barrier, inc=1, device_id=z_peer(k)[1], device_id_type=MESH)
    for k in range(1, NDP):
        pl.semaphore_signal(barrier, inc=1, device_id=dp_peer(k)[1], device_id_type=MESH)
    for k in range(1, NY):
        pl.semaphore_signal(barrier, inc=1, device_id=y_peer(k)[1], device_id_type=MESH)

    loads = [pltpu.make_async_copy(tok_hbm, hid.at[0], load_sem.at[0])]
    for l in range(2):
        for p, w in enumerate((wr, wk, wv, wd, wa, wg)):
            loads.append(
                pltpu.make_async_copy(w.at[l], wt.at[l, pl.ds(64 * p, 64)], load_sem.at[1 + 6 * l + p])
            )
    state_loads = [pltpu.make_async_copy(st_hbm.at[l], st.at[l], load_sem.at[13 + l]) for l in range(2)]
    wo_loads = [pltpu.make_async_copy(wo_hbm.at[l], wo.at[l, yi], load_sem.at[15 + 5 * l]) for l in range(2)]
    smalls = [
        pltpu.make_async_copy(a, b, load_sem.at[16 + i])
        for i, (a, b) in enumerate(
            ((gain_hbm, gain_ref), (floor_hbm, floor_ref), (direct_hbm, direct_ref), (norm_hbm, norm_ref))
        )
    ]
    loads[0].start()
    for cp in smalls:
        cp.start()
    for cp in loads[1:7]:
        cp.start()
    state_loads[0].start()
    wo_loads[0].start()
    for cp in loads[7:]:
        cp.start()
    state_loads[1].start()
    wo_loads[1].start()

    for l in range(2):
        if l == 0:
            loads[0].wait()
            for cp in smalls:
                cp.wait()
        for cp in loads[1 + 6 * l : 7 + 6 * l]:
            cp.wait()
        hv = hid[l].astype(F32).reshape(NZ, 4, 8, 128)
        sq = None
        xs = []
        for cg in range(4):
            part = hv[:, cg].reshape(256, 128)
            sq = part * part if sq is None else sq + part * part
            xs.append((part * gain_ref[l : l + 1, 128 * cg : 128 * cg + 128]).astype(BF16))
        high = sq.astype(BF16)
        ones = jnp.ones((8, 128), BF16)
        sums = lax.dot_general(ones, high, NT, preferred_element_type=F32) + lax.dot_general(
            ones, (sq - high.astype(F32)).astype(BF16), NT, preferred_element_type=F32
        )
        high = sums.astype(BF16).astype(F32)
        sums = jnp.where(lax.broadcasted_iota(jnp.int32, (8, 256), 0) == 0, high, sums - high).astype(BF16)
        tsend[l, 0] = sums[:, 0:128]
        tsend[l, 1] = sums[:, 128:256]
        proj = lax.dot_general(
            jnp.concatenate(xs, axis=1), wt[l], NT, preferred_element_type=F32
        ).astype(BF16)
        psend[l] = proj.reshape(NDP, SEQ, 384)
        if l == 0:
            with jax.named_scope("w_bar"):
                pl.semaphore_wait(barrier, 8 + (NDP - 1) + (NY - 1))
            for k in (4, NZ - 4):
                pl.semaphore_signal(within8, inc=1, device_id=z_peer(k)[1], device_id_type=MESH)
        for k in (4, 3, 5, 2, 6, 1, 7):
            d, dev = dp_peer(k)
            remote(tsend.at[l, lax.div(d, 4)], trecv.at[l, di], t_ss.at[l], t_rs.at[l], dev).start()
        for k in (4, 3, 5, 2, 6, 1, 7):
            d, dev = dp_peer(k)
            remote(psend.at[l, d], precv.at[l, di], p_ss.at[l], p_rs.at[l], dev).start()
        if l == 0:
            wo_loads[0].wait()
            for k in (2, 1, 3):
                remote(wo.at[0, yi], wo.at[0, yi], w_ss.at[0], w_rs.at[0], y_peer(k)[1]).start()
        with jax.named_scope("w_st"):
            state_loads[l].wait()
        stb[...] = st[l].reshape(SEQ * HC, HC).astype(BF16)
        if l == 0:
            with jax.named_scope("w_8"):
                pl.semaphore_wait(within8, 2)
            for k in (8, NZ - 8):
                pl.semaphore_signal(within16, inc=1, device_id=z_peer(k)[1], device_id_type=MESH)
        total = psend[l, di].astype(F32)
        with jax.named_scope("w_p"):
            remote(
                psend.at[l, pl.ds(0, NDP - 1)], precv.at[l, pl.ds(0, NDP - 1)], p_ss.at[l], p_rs.at[l], {"y": lax.rem(yi + 1, NY)}
            ).wait_recv()
        for k in range(1, NDP):
            total = total + precv[l, lax.rem(di + k, NDP)].astype(F32)
        some = trecv.at[l, pl.ds(0, NDP - 1)]
        remote(some, some, t_ss.at[l], t_rs.at[l], y_peer(1)[1]).wait_recv()
        squares = tsend[l, lax.div(di, 4)].astype(F32)
        for k in range(1, NDP):
            squares = squares + trecv[l, lax.rem(di + k, NDP)].astype(F32)
        squares = squares[0:1] + squares[1:2]
        picked = lax.broadcasted_iota(jnp.int32, (SEQ, 128), 1) == (
            lax.broadcasted_iota(jnp.int32, (SEQ, 128), 0) + SEQ * lax.rem(di, 4)
        )
        squares = jnp.sum(jnp.where(picked, squares, 0.0), axis=1, keepdims=True)
        total = total * lax.rsqrt(squares * (1.0 / D) + 1e-6)
        r, k_, v, pd, pa, pg = [total[:, 64 * p : 64 * p + 64] for p in range(6)]
        decay = jnp.exp(-0.6065306597126334 * jax.nn.sigmoid(floor_ref[l : l + 1, :] + pd))
        rate = jax.nn.sigmoid(pa)
        gate = jax.nn.sigmoid(pg)
        u = k_ * lax.rsqrt(jnp.sum(k_ * k_, axis=1, keepdims=True) + 1e-6)
        kr = k_ * rate
        ur = u * rate
        dr = decay * r
        row16 = lax.broadcasted_iota(jnp.int32, (16, 64), 0) % 8
        cs, ys = [], []
        for q in range(4):
            rows = slice(8 * q, 8 * q + 8)
            left = jnp.concatenate([u[rows], dr[rows]], axis=0).astype(BF16)
            res = lax.dot_general(left, stb[512 * q : 512 * q + 512], NT, preferred_element_type=F32)
            acc = jnp.zeros((16, 64), F32)
            for t in range(8):
                acc = jnp.where(row16 == t, res[:, 64 * t : 64 * t + 64], acc)
            cs.append(acc[0:8])
            ys.append(acc[8:16])
        c = -jnp.concatenate(cs, axis=0)
        y = (
            jnp.concatenate(ys, axis=0)
            + c * jnp.sum(ur * r, axis=1, keepdims=True)
            + v * jnp.sum(kr * r, axis=1, keepdims=True)
        )
        y = y - jnp.mean(y, axis=1, keepdims=True)
        var = jnp.mean(y * y, axis=1, keepdims=True)
        o = y * lax.rsqrt(var + 0.00064) * norm_ref[l : l + 1, :]
        o = o + jnp.sum(r * kr * direct_ref[l : l + 1, :], axis=1, keepdims=True) * v
        o = o * gate
        osend[l] = jnp.concatenate([o[0:16], o[16:32]], axis=1).astype(BF16)
        slot = yi * NC + ci
        for k in (4, 3, 5, 2, 6, 1, 7):
            remote(osend.at[l], oget.at[l, slot], o_ss.at[l], o_rs.at[l], {**dp_peer(k)[1], "y": xi}).start()

        @pl.when(yi != xi)
        def _():
            remote(osend.at[l], oget.at[l, slot], o_ss.at[l], o_rs.at[l], {"y": xi}).start()

        @pl.when(yi == xi)
        def _():
            oget[l, slot] = osend[l]

        if l == 0:
            wo_loads[1].wait()
            for k in (2, 1, 3):
                remote(wo.at[1, yi], wo.at[1, yi], w_ss.at[1], w_rs.at[1], y_peer(k)[1]).start()
        ct = c.T
        vt = v.T

        def update(lo, hi):
            for s in range(lo, hi):
                st_out[l, s] = (
                    st[l, s] * decay[s : s + 1, :]
                    + ct[:, s : s + 1] * ur[s : s + 1, :]
                    + vt[:, s : s + 1] * kr[s : s + 1, :]
                )

        with jax.named_scope("w_w"):
            some = wo.at[l, pl.ds(0, 3)]
            remote(some, some, w_ss.at[l], w_rs.at[l], y_peer(1)[1]).wait_recv()
        with jax.named_scope("w_o"):
            o_count(l, lambda some: remote(some, some, o_ss.at[l], o_rs.at[l], y_peer(1)[1]).wait_recv())

        left = []
        for p in range(NY):
            packed = [oget[l, p * NC + i] for i in range(NC)]
            left.append(jnp.concatenate([b[:, c0 : c0 + 64] for b in packed for c0 in (0, 64)], axis=0))
        share = lax.dot_general(
            jnp.concatenate(left, axis=1), wo[l].reshape(NY * HC, 512), NN, preferred_element_type=F32
        ).astype(BF16)
        for rg in range(8):
            for cg in range(4):
                zsend[l, order[rg % 4 * 4 + cg], rg // 4] = share[8 * rg : 8 * rg + 8, 128 * cg : 128 * cg + 128]
        if l == 0:
            with jax.named_scope("w_16"):
                pl.semaphore_wait(within16, 2)

        def z_scatter(k, _):
            src = zsend.at[l, jnp.where(k < 16, k, 31 - k)]
            remote(src, zrecv.at[l, zi], z_ss.at[l], z_rs.at[l], z_peer(far_first(k))[1]).start()
            return 0

        with jax.named_scope("zsend"):
            lax.fori_loop(0, NZ - 1, z_scatter, 0)
        zrecv[l, zi] = zsend[l, 0]
        with jax.named_scope("upd"):
            update(0, SEQ)
        with jax.named_scope("w_z"):
            some = zrecv.at[l, pl.ds(0, NZ - 1)]
            remote(some, some, z_ss.at[l], z_rs.at[l], z_peer(1)[1]).wait_recv()
        def pair(at):
            return hid.at[l + 1, yi, :, lax.rem(at, 16)]

        mine = jnp.sum(zrecv[l].astype(F32), axis=0)
        for h in range(2):
            hid[l + 1, yi, h, lax.rem(zi, 16)] = (mine[h] + hid[l, yi, h, lax.rem(zi, 16)].astype(F32)).astype(BF16)

        for g, (lo, hi) in enumerate(GROUPS):

            def z_gather(k, _):
                _, dev = z_peer(near_off(k))
                remote(pair(zi), pair(zi), g_ss.at[l], g_rs.at[l, g], dev).start()
                if g < DIRECT:
                    for i in (2, 1, 3):
                        both = {**dev, **y_peer(i)[1]}
                        remote(pair(zi), pair(zi), h_ss.at[l], h_rs.at[l], both).start()
                return 0

            with jax.named_scope("zsend"):
                lax.fori_loop(lo, hi, z_gather, 0)

        def forward(at):
            for k in (2, 1, 3):
                remote(pair(at), pair(at), h_ss.at[l], h_rs.at[l], y_peer(k)[1]).start()

        forward(zi)
        for g in range(len(GROUPS) - 1, -1, -1):
            lo, hi = GROUPS[g]
            with jax.named_scope("w_g"):
                some = zsend.at[l, pl.ds(0, hi - lo)]
                remote(some, some, g_ss.at[l], g_rs.at[l, g], z_peer(1)[1]).wait_recv()

            def onward(k, _):
                forward(zi + NZ - near_off(k))
                return 0

            if g >= DIRECT:
                with jax.named_scope("fwd"):
                    lax.fori_loop(lo, hi, onward, 0)
        three = hid.at[l + 1, pl.ds(0, 3)]
        with jax.named_scope("w_h"):
            remote(three, three, h_ss.at[l], h_rs.at[l], {"y": lax.rem(yi + 1, NY)}).wait_recv()

    hid_out[...] = hid[2]
    for l in range(2):
        near = {"y": lax.rem(yi + 1, NY)}
        for buf, ss in (
            (trecv.at[l, pl.ds(0, NDP - 1)], t_ss),
            (psend.at[l, pl.ds(0, NDP - 1)], p_ss),
            (wo.at[l, pl.ds(0, 3)], w_ss),
            (zrecv.at[l, pl.ds(0, NZ - 1)], z_ss),
            (zsend.at[l, pl.ds(0, 15)], g_ss),
            (hid.at[l, pl.ds(0, 3)], h_ss),
        ):
            remote(buf, buf, ss.at[l], p_rs.at[l], near).wait_send()
        o_count(l, lambda some: remote(some, some, o_ss.at[l], o_rs.at[l], near).wait_send())


def per_device(
    incoming_token, input_norm_gain, receptance_weight, key_weight, value_weight, decay_weight,
    learning_rate_weight, gate_weight, channel_decay_floor, direct_token_weight, head_norm_gain,
    output_weight, incoming_state,
):
    tiles = incoming_token.reshape(NZ, 8, 4, 128).transpose(0, 2, 1, 3).reshape(NY, 2, 16, 8, 128)
    weights = [
        jnp.swapaxes(w, 1, 2)
        for w in (
            receptance_weight, key_weight, value_weight, decay_weight, learning_rate_weight, gate_weight,
        )
    ]
    state = incoming_state.reshape(2, SEQ, HC, HC)
    anywhere = pl.BlockSpec(memory_space=pl.ANY)
    vmem = pl.BlockSpec(memory_space=pltpu.VMEM)
    dma = pltpu.SemaphoreType.DMA
    hidden, new_state = pl.pallas_call(
        kernel,
        out_shape=(
            pltpu.VMEM((NY, 2, 16, 8, 128), BF16),
            pltpu.VMEM((2, SEQ, HC, HC), F32),
        ),
        in_specs=[anywhere] * 13,
        out_specs=(vmem, vmem),
        scratch_shapes=[
            pltpu.VMEM((3, NY, 2, 16, 8, 128), BF16),
            pltpu.VMEM((2, 512), F32),
            *[pltpu.VMEM((2, HC), F32) for _ in range(3)],
            pltpu.VMEM((2, 384, 512), BF16),
            pltpu.VMEM((2, NY, HC, 512), BF16),
            pltpu.VMEM((2, SEQ, HC, HC), F32),
            pltpu.VMEM((SEQ * HC, HC), BF16),
            pltpu.VMEM((2, 2, 8, 128), BF16),
            pltpu.VMEM((2, NDP, 8, 128), BF16),
            pltpu.VMEM((2, NDP, SEQ, 384), BF16),
            pltpu.VMEM((2, NDP, SEQ, 384), BF16),
            pltpu.VMEM((2, 16, 128), BF16),
            pltpu.VMEM((2, NY * NC, 16, 128), BF16),
            pltpu.VMEM((2, 16, 2, 8, 128), BF16),
            pltpu.VMEM((2, NZ, 2, 8, 128), BF16),
            dma((21,)),
            *[dma((2,)) for _ in range(11)],
            dma((2, len(GROUPS))),
            *[dma((2,)) for _ in range(2)],
            pltpu.SemaphoreType.REGULAR,
            pltpu.SemaphoreType.REGULAR,
        ],
        compiler_params=pltpu.CompilerParams(
            collective_id=0, has_side_effects=True, vmem_limit_bytes=60 * 1024 * 1024
        ),
        name="decode_step",
    )(
        tiles, input_norm_gain, *weights, channel_decay_floor, direct_token_weight, head_norm_gain,
        output_weight, state,
    )
    hidden = hidden.reshape(NZ, 4, 8, 128).transpose(0, 2, 1, 3).reshape(256, 512)
    return (hidden, new_state.reshape(2, SEQ, 1, HC, HC))


def solution(mesh):
    finer = Mesh(mesh.devices.reshape(NZ, NY, NX, NC), ("z", "y", "x", "c"))
    tp, dp = ("z", "y"), ("x", "c")
    w = P(None, dp, tp)
    return jax.shard_map(
        per_device,
        mesh=finer,
        in_specs=(
            P(None, dp), P(None, dp), w, w, w, w, w, w, P(None, tp), P(None, tp), P(None, tp),
            P(None, tp, dp), P(None, dp, tp, None, None),
        ),
        out_specs=(P(None, dp), P(None, dp, tp, None, None)),
        check_vma=False,
    )
```

```python
import functools

import jax
import jax.numpy as jnp
from jax import lax
from jax.experimental import pallas as pl
from jax.experimental.pallas import tpu as pltpu
from jax.sharding import Mesh
from jax.sharding import PartitionSpec as P

MESH = pl.DeviceIdType.MESH
F32 = jnp.float32
BF16 = jnp.bfloat16
NZ, NY, NX, NC = 32, 4, 4, 2
NDP = NX * NC
D = 4096
HC = 64
SEQ = 32
NT = (((1,), (1,)), ((), ()))
NN = (((1,), (0,)), ((), ()))
GROUPS = ((0, 3), (3, 7), (7, 11), (11, 15))
DIRECT = 0


def kernel(
    tok_hbm, gain_hbm, wr, wk, wv, wd, wa, wg, floor_hbm, direct_hbm, norm_hbm, wo_hbm, st_hbm,
    hid_out, st_out,
    hid, gain_ref, floor_ref, direct_ref, norm_ref, wt, wo, st, stb, tsend, trecv, psend, precv, osend, oget, zsend, zrecv,
    load_sem, t_ss, t_rs, p_ss, p_rs, o_ss, o_rs, w_ss, w_rs, z_ss, z_rs, g_ss, g_rs, h_ss, h_rs, m_sem, within8, within16,
):
    zi, yi = lax.axis_index("z"), lax.axis_index("y")
    xi, ci = lax.axis_index("x"), lax.axis_index("c")
    di = xi * NC + ci
    odd = lax.rem(zi, 2)
    mate = {"z": zi + 1 - 2 * odd}
    place = lax.div(zi, 2)
    own_head, mate_head = odd * NY + yi, (1 - odd) * NY + yi

    def dp_peer(k):
        d = lax.rem(di + k, NDP)
        return d, {"x": lax.div(d, NC), "c": lax.rem(d, NC)}

    def y_peer(k):
        p = lax.rem(yi + k, NY)
        return p, {"y": p}

    def z_peer(k):
        p = lax.rem(zi + k, NZ)
        return p, {"z": p}

    def remote(src, dst, ss, rs, dev):
        return pltpu.make_async_remote_copy(
            src_ref=src, dst_ref=dst, send_sem=ss, recv_sem=rs, device_id=dev, device_id_type=MESH
        )

    def far_first(k):
        return jnp.where(k % 2 == 0, 8 + k // 2, 8 - (k + 1) // 2)

    def near_off(k):
        return jnp.where(k % 2 == 0, NZ - 8 + k // 2, 8 - (k + 1) // 2)

    def wo_gather():
        own = wo.at[0, own_head]
        for dev in (y_peer(2)[1], {**y_peer(2)[1], **mate}, mate, *[{**y_peer(k)[1], **m} for k in (1, 3) for m in ({}, mate)]):
            remote(own, own, w_ss.at[0], w_rs.at[0], dev).start()

    o_home = (yi == xi) & (odd == ci)

    def o_count(l, wait):
        @pl.when(jnp.logical_not(o_home))
        def _():
            wait(oget.at[l])

        @pl.when(o_home)
        def _():
            wait(oget.at[l, pl.ds(0, NDP - 1)])

    barrier = pltpu.get_barrier_semaphore()

    for k in (1, 2, 3, 4, NZ - 4, NZ - 3, NZ - 2, NZ - 1):
        pl.semaphore_signal(barrier, inc=1, device_id=z_peer(k)[1], device_id_type=MESH)
    for k in range(1, NDP):
        pl.semaphore_signal(barrier, inc=1, device_id=dp_peer(k)[1], device_id_type=MESH)
    for k in range(1, NY):
        pl.semaphore_signal(barrier, inc=1, device_id=y_peer(k)[1], device_id_type=MESH)
        pl.semaphore_signal(barrier, inc=1, device_id={**y_peer(k)[1], **mate}, device_id_type=MESH)

    to_mate = remote(wo.at[1, own_head], wo.at[1, own_head], m_sem.at[0], m_sem.at[1], mate)

    loads = [pltpu.make_async_copy(tok_hbm, hid.at[0], load_sem.at[0])]
    for l in range(2):
        for p, w in enumerate((wr, wk, wv, wd, wa, wg)):
            loads.append(
                pltpu.make_async_copy(w.at[l], wt.at[l, pl.ds(64 * p, 64)], load_sem.at[1 + 6 * l + p])
            )
    state_loads = [pltpu.make_async_copy(st_hbm.at[l], st.at[l], load_sem.at[13 + l]) for l in range(2)]
    wo_loads = [pltpu.make_async_copy(wo_hbm.at[l], wo.at[l, own_head], load_sem.at[15 + 5 * l]) for l in range(2)]
    smalls = [
        pltpu.make_async_copy(a, b, load_sem.at[16 + i])
        for i, (a, b) in enumerate(
            ((gain_hbm, gain_ref), (floor_hbm, floor_ref), (direct_hbm, direct_ref), (norm_hbm, norm_ref))
        )
    ]
    loads[0].start()
    for cp in smalls:
        cp.start()
    for cp in loads[1:7]:
        cp.start()
    state_loads[0].start()
    wo_loads[0].start()
    for cp in loads[7:]:
        cp.start()
    state_loads[1].start()
    wo_loads[1].start()

    for l in range(2):
        if l == 0:
            loads[0].wait()
            for cp in smalls:
                cp.wait()
        for cp in loads[1 + 6 * l : 7 + 6 * l]:
            cp.wait()
        hv = hid[l].astype(F32).reshape(NZ, 4, 8, 128)
        sq = None
        xs = []
        for cg in range(4):
            part = hv[:, cg].reshape(256, 128)
            sq = part * part if sq is None else sq + part * part
            xs.append((part * gain_ref[l : l + 1, 128 * cg : 128 * cg + 128]).astype(BF16))
        high = sq.astype(BF16)
        ones = jnp.ones((8, 128), BF16)
        sums = lax.dot_general(ones, high, NT, preferred_element_type=F32) + lax.dot_general(
            ones, (sq - high.astype(F32)).astype(BF16), NT, preferred_element_type=F32
        )
        high = sums.astype(BF16).astype(F32)
        sums = jnp.where(lax.broadcasted_iota(jnp.int32, (8, 256), 0) == 0, high, sums - high).astype(BF16)
        tsend[l, 0] = sums[:, 0:128]
        tsend[l, 1] = sums[:, 128:256]
        proj = lax.dot_general(
            jnp.concatenate(xs, axis=1), wt[l], NT, preferred_element_type=F32
        ).astype(BF16)
        psend[l] = proj.reshape(NDP, SEQ, 384)
        if l == 0:
            with jax.named_scope("w_bar"):
                pl.semaphore_wait(barrier, 8 + (NDP - 1) + 2 * (NY - 1))
            wo_loads[0].wait()
            wo_gather()
            for k in (4, NZ - 4):
                pl.semaphore_signal(within8, inc=1, device_id=z_peer(k)[1], device_id_type=MESH)
        for k in (4, 3, 5, 2, 6, 1, 7):
            d, dev = dp_peer(k)
            remote(tsend.at[l, lax.div(d, 4)], trecv.at[l, di], t_ss.at[l], t_rs.at[l], dev).start()
        for k in (4, 3, 5, 2, 6, 1, 7):
            d, dev = dp_peer(k)
            remote(psend.at[l, d], precv.at[l, di], p_ss.at[l], p_rs.at[l], dev).start()
        if l == 0:
            wo_loads[1].wait()
            to_mate.start()
        with jax.named_scope("w_st"):
            state_loads[l].wait()
        stb[...] = st[l].reshape(SEQ * HC, HC).astype(BF16)
        if l == 0:
            with jax.named_scope("w_8"):
                pl.semaphore_wait(within8, 2)
            for k in (8, NZ - 8):
                pl.semaphore_signal(within16, inc=1, device_id=z_peer(k)[1], device_id_type=MESH)
        total = psend[l, di].astype(F32)
        with jax.named_scope("w_p"):
            remote(
                psend.at[l, pl.ds(0, NDP - 1)], precv.at[l, pl.ds(0, NDP - 1)], p_ss.at[l], p_rs.at[l], {"y": lax.rem(yi + 1, NY)}
            ).wait_recv()
        for k in range(1, NDP):
            total = total + precv[l, lax.rem(di + k, NDP)].astype(F32)
        some = trecv.at[l, pl.ds(0, NDP - 1)]
        remote(some, some, t_ss.at[l], t_rs.at[l], y_peer(1)[1]).wait_recv()
        squares = tsend[l, lax.div(di, 4)].astype(F32)
        for k in range(1, NDP):
            squares = squares + trecv[l, lax.rem(di + k, NDP)].astype(F32)
        squares = squares[0:1] + squares[1:2]
        picked = lax.broadcasted_iota(jnp.int32, (SEQ, 128), 1) == (
            lax.broadcasted_iota(jnp.int32, (SEQ, 128), 0) + SEQ * lax.rem(di, 4)
        )
        squares = jnp.sum(jnp.where(picked, squares, 0.0), axis=1, keepdims=True)
        total = total * lax.rsqrt(squares * (1.0 / D) + 1e-6)
        r, k_, v, pd, pa, pg = [total[:, 64 * p : 64 * p + 64] for p in range(6)]
        decay = jnp.exp(-0.6065306597126334 * jax.nn.sigmoid(floor_ref[l : l + 1, :] + pd))
        rate = jax.nn.sigmoid(pa)
        gate = jax.nn.sigmoid(pg)
        u = k_ * lax.rsqrt(jnp.sum(k_ * k_, axis=1, keepdims=True) + 1e-6)
        kr = k_ * rate
        ur = u * rate
        dr = decay * r
        row16 = lax.broadcasted_iota(jnp.int32, (16, 64), 0) % 8
        cs, ys = [], []
        for q in range(4):
            rows = slice(8 * q, 8 * q + 8)
            left = jnp.concatenate([u[rows], dr[rows]], axis=0).astype(BF16)
            res = lax.dot_general(left, stb[512 * q : 512 * q + 512], NT, preferred_element_type=F32)
            acc = jnp.zeros((16, 64), F32)
            for t in range(8):
                acc = jnp.where(row16 == t, res[:, 64 * t : 64 * t + 64], acc)
            cs.append(acc[0:8])
            ys.append(acc[8:16])
        c = -jnp.concatenate(cs, axis=0)
        y = (
            jnp.concatenate(ys, axis=0)
            + c * jnp.sum(ur * r, axis=1, keepdims=True)
            + v * jnp.sum(kr * r, axis=1, keepdims=True)
        )
        y = y - jnp.mean(y, axis=1, keepdims=True)
        var = jnp.mean(y * y, axis=1, keepdims=True)
        o = y * lax.rsqrt(var + 0.00064) * norm_ref[l : l + 1, :]
        o = o + jnp.sum(r * kr * direct_ref[l : l + 1, :], axis=1, keepdims=True) * v
        o = o * gate
        osend[l] = jnp.concatenate([o[0:16], o[16:32]], axis=1).astype(BF16)
        there = {"y": xi, "z": zi - odd + ci}
        for k in (4, 3, 5, 2, 6, 1, 7):
            remote(osend.at[l], oget.at[l, own_head], o_ss.at[l], o_rs.at[l], {**dp_peer(k)[1], **there}).start()

        @pl.when(jnp.logical_not(o_home))
        def _():
            remote(osend.at[l], oget.at[l, own_head], o_ss.at[l], o_rs.at[l], there).start()

        @pl.when(o_home)
        def _():
            oget[l, own_head] = osend[l]

        ct = c.T
        vt = v.T

        def update(lo, hi):
            for s in range(lo, hi):
                st_out[l, s] = (
                    st[l, s] * decay[s : s + 1, :]
                    + ct[:, s : s + 1] * ur[s : s + 1, :]
                    + vt[:, s : s + 1] * kr[s : s + 1, :]
                )

        with jax.named_scope("w_w"):
            some = wo.at[l, pl.ds(0, 7 - l)]
            remote(some, some, w_ss.at[l], w_rs.at[l], y_peer(1)[1]).wait_recv()
        with jax.named_scope("w_o"):
            o_count(l, lambda some: remote(some, some, o_ss.at[l], o_rs.at[l], y_peer(1)[1]).wait_recv())

        left = []
        for p in range(2 * NY):
            packed = oget[l, p]
            left.append(jnp.concatenate([packed[:, 0:64], packed[:, 64:128]], axis=0))
        share = lax.dot_general(
            jnp.concatenate(left, axis=1), wo[l].reshape(2 * NY * HC, 512), NN, preferred_element_type=F32
        ).astype(BF16)
        for n in range(16):
            rg, cg = n // 4, n % 4
            zsend[l, n % 8, n // 8] = share[8 * rg : 8 * rg + 8, 128 * cg : 128 * cg + 128]
        if l == 0:
            with jax.named_scope("w_16"):
                pl.semaphore_wait(within16, 2)

        def z_scatter(k, _):
            p, dev = z_peer(2 * far_first(k))
            src = zsend.at[l, lax.rem(lax.div(p, 2), 8)]
            remote(src, zrecv.at[l, place], z_ss.at[l], z_rs.at[l], dev).start()
            return 0

        with jax.named_scope("zsend"):
            lax.fori_loop(0, 15, z_scatter, 0)
        if l == 0:
            to_mate.wait_recv()
            for k in (2, 1, 3):
                for head in (own_head, mate_head):
                    remote(wo.at[1, head], wo.at[1, head], w_ss.at[1], w_rs.at[1], y_peer(k)[1]).start()
        zrecv[l, place] = zsend[l, lax.rem(place, 8)]
        with jax.named_scope("upd"):
            update(0, SEQ)
        with jax.named_scope("w_z"):
            some = zrecv.at[l, pl.ds(0, 15)]
            remote(some, some, z_ss.at[l], z_rs.at[l], z_peer(1)[1]).wait_recv()
        def pair(at):
            return hid.at[l + 1, yi, lax.rem(at, 2), :, lax.rem(lax.div(at, 2), 8)]

        mine = jnp.sum(zrecv[l].astype(F32), axis=0)
        for h in range(2):
            q = lax.rem(place, 8)
            hid[l + 1, yi, odd, h, q] = (mine[h] + hid[l, yi, odd, h, q].astype(F32)).astype(BF16)

        for g, (lo, hi) in enumerate(GROUPS):

            def z_gather(k, _):
                _, dev = z_peer(near_off(k))
                remote(pair(zi), pair(zi), g_ss.at[l], g_rs.at[l, g], dev).start()
                if g < DIRECT:
                    for i in (2, 1, 3):
                        both = {**dev, **y_peer(i)[1]}
                        remote(pair(zi), pair(zi), h_ss.at[l], h_rs.at[l], both).start()
                return 0

            with jax.named_scope("zsend"):
                lax.fori_loop(lo, hi, z_gather, 0)

        def forward(at):
            for k in (2, 1, 3):
                remote(pair(at), pair(at), h_ss.at[l], h_rs.at[l], y_peer(k)[1]).start()

        forward(zi)
        for g in range(len(GROUPS) - 1, -1, -1):
            lo, hi = GROUPS[g]
            with jax.named_scope("w_g"):
                some = zrecv.at[l, pl.ds(0, hi - lo)]
                remote(some, some, g_ss.at[l], g_rs.at[l, g], z_peer(1)[1]).wait_recv()

            def onward(k, _):
                forward(zi + NZ - near_off(k))
                return 0

            if g >= DIRECT:
                with jax.named_scope("fwd"):
                    lax.fori_loop(lo, hi, onward, 0)
        three = hid.at[l + 1, pl.ds(0, 3)]
        with jax.named_scope("w_h"):
            remote(three, three, h_ss.at[l], h_rs.at[l], {"y": lax.rem(yi + 1, NY)}).wait_recv()

    hid_out[...] = hid[2]
    to_mate.wait_send()
    for l in range(2):
        near = {"y": lax.rem(yi + 1, NY)}
        for buf, ss in (
            (trecv.at[l, pl.ds(0, NDP - 1)], t_ss),
            (psend.at[l, pl.ds(0, NDP - 1)], p_ss),
            (wo.at[l, pl.ds(0, 7 - l)], w_ss),
            (zrecv.at[l, pl.ds(0, 15)], z_ss),
            (zrecv.at[l, pl.ds(0, 15)], g_ss),
            (hid.at[l, pl.ds(0, 3)], h_ss),
        ):
            remote(buf, buf, ss.at[l], p_rs.at[l], near).wait_send()
        o_count(l, lambda some: remote(some, some, o_ss.at[l], o_rs.at[l], near).wait_send())


def per_device(
    incoming_token, input_norm_gain, receptance_weight, key_weight, value_weight, decay_weight,
    learning_rate_weight, gate_weight, channel_decay_floor, direct_token_weight, head_norm_gain,
    output_weight, incoming_state,
):
    tiles = incoming_token.reshape(NZ, 8, 4, 128).transpose(0, 2, 1, 3).reshape(NY, 2, 2, 8, 8, 128)
    weights = [
        jnp.swapaxes(w, 1, 2)
        for w in (
            receptance_weight, key_weight, value_weight, decay_weight, learning_rate_weight, gate_weight,
        )
    ]
    state = incoming_state.reshape(2, SEQ, HC, HC)
    anywhere = pl.BlockSpec(memory_space=pl.ANY)
    vmem = pl.BlockSpec(memory_space=pltpu.VMEM)
    dma = pltpu.SemaphoreType.DMA
    hidden, new_state = pl.pallas_call(
        kernel,
        out_shape=(
            pltpu.VMEM((NY, 2, 2, 8, 8, 128), BF16),
            pltpu.VMEM((2, SEQ, HC, HC), F32),
        ),
        in_specs=[anywhere] * 13,
        out_specs=(vmem, vmem),
        scratch_shapes=[
            pltpu.VMEM((3, NY, 2, 2, 8, 8, 128), BF16),
            pltpu.VMEM((2, 512), F32),
            *[pltpu.VMEM((2, HC), F32) for _ in range(3)],
            pltpu.VMEM((2, 384, 512), BF16),
            pltpu.VMEM((2, 2 * NY, HC, 512), BF16),
            pltpu.VMEM((2, SEQ, HC, HC), F32),
            pltpu.VMEM((SEQ * HC, HC), BF16),
            pltpu.VMEM((2, 2, 8, 128), BF16),
            pltpu.VMEM((2, NDP, 8, 128), BF16),
            pltpu.VMEM((2, NDP, SEQ, 384), BF16),
            pltpu.VMEM((2, NDP, SEQ, 384), BF16),
            pltpu.VMEM((2, 16, 128), BF16),
            pltpu.VMEM((2, NY * NC, 16, 128), BF16),
            pltpu.VMEM((2, 8, 2, 8, 128), BF16),
            pltpu.VMEM((2, 16, 2, 8, 128), BF16),
            dma((21,)),
            *[dma((2,)) for _ in range(11)],
            dma((2, len(GROUPS))),
            *[dma((2,)) for _ in range(2)],
            dma((2,)),
            pltpu.SemaphoreType.REGULAR,
            pltpu.SemaphoreType.REGULAR,
        ],
        compiler_params=pltpu.CompilerParams(
            collective_id=0, has_side_effects=True, vmem_limit_bytes=60 * 1024 * 1024
        ),
        name="decode_step",
    )(
        tiles, input_norm_gain, *weights, channel_decay_floor, direct_token_weight, head_norm_gain,
        output_weight, state,
    )
    hidden = hidden.reshape(NZ, 4, 8, 128).transpose(0, 2, 1, 3).reshape(256, 512)
    return (hidden, new_state.reshape(2, SEQ, 1, HC, HC))


def solution(mesh):
    finer = Mesh(mesh.devices.reshape(NZ, NY, NX, NC), ("z", "y", "x", "c"))
    tp, dp = ("z", "y"), ("x", "c")
    w = P(None, dp, tp)
    return jax.shard_map(
        per_device,
        mesh=finer,
        in_specs=(
            P(None, dp), P(None, dp), w, w, w, w, w, w, P(None, tp), P(None, tp), P(None, tp),
            P(None, tp, dp), P(None, dp, tp, None, None),
        ),
        out_specs=(P(None, dp), P(None, dp, tp, None, None)),
        check_vma=False,
    )
```

```python
import functools

import jax
import jax.numpy as jnp
from jax import lax
from jax.experimental import pallas as pl
from jax.experimental.pallas import tpu as pltpu
from jax.sharding import Mesh
from jax.sharding import PartitionSpec as P

MESH = pl.DeviceIdType.MESH
F32 = jnp.float32
BF16 = jnp.bfloat16
NZ, NY, NX, NC = 32, 4, 4, 2
NDP = NX * NC
D = 4096
HC = 64
SEQ = 32
NT = (((1,), (1,)), ((), ()))
NN = (((1,), (0,)), ((), ()))
GROUPS = ((0, 3), (3, 7), (7, 11), (11, 15))
DIRECT = 0


def kernel(
    tok_hbm, gain_hbm, wr, wk, wv, wd, wa, wg, floor_hbm, direct_hbm, norm_hbm, wo_hbm, st_hbm,
    hid_out, st_out,
    hid, gain_ref, floor_ref, direct_ref, norm_ref, wt, wo, st, stb, tsend, trecv, psend, precv, osend, oget, zsend, zrecv,
    load_sem, t_ss, t_rs, p_ss, p_rs, o_ss, o_rs, w_ss, w_rs, z_ss, z_rs, g_ss, g_rs, h_ss, h_rs, m_sem, within8, within16,
):
    zi, yi = lax.axis_index("z"), lax.axis_index("y")
    xi, ci = lax.axis_index("x"), lax.axis_index("c")
    di = xi * NC + ci
    odd = lax.rem(zi, 2)
    mate = {"z": zi + 1 - 2 * odd}
    place = lax.div(zi, 2)
    own_head, mate_head = odd * NY + yi, (1 - odd) * NY + yi

    def dp_peer(k):
        d = lax.rem(di + k, NDP)
        return d, {"x": lax.div(d, NC), "c": lax.rem(d, NC)}

    def y_peer(k):
        p = lax.rem(yi + k, NY)
        return p, {"y": p}

    def z_peer(k):
        p = lax.rem(zi + k, NZ)
        return p, {"z": p}

    def remote(src, dst, ss, rs, dev):
        return pltpu.make_async_remote_copy(
            src_ref=src, dst_ref=dst, send_sem=ss, recv_sem=rs, device_id=dev, device_id_type=MESH
        )

    def far_first(k):
        return jnp.where(k % 2 == 0, 8 + k // 2, 8 - (k + 1) // 2)

    def near_off(k):
        return jnp.where(k % 2 == 0, NZ - 8 + k // 2, 8 - (k + 1) // 2)

    def wo_gather():
        own = wo.at[0, own_head]
        for dev in (y_peer(2)[1], {**y_peer(2)[1], **mate}, mate, *[{**y_peer(k)[1], **m} for k in (1, 3) for m in ({}, mate)]):
            remote(own, own, w_ss.at[0], w_rs.at[0], dev).start()

    o_home = (yi == xi) & (odd == ci)

    def o_count(l, wait):
        @pl.when(jnp.logical_not(o_home))
        def _():
            wait(oget.at[l])

        @pl.when(o_home)
        def _():
            wait(oget.at[l, pl.ds(0, NDP - 1)])

    barrier = pltpu.get_barrier_semaphore()

    for k in (1, 2, 3, 4, NZ - 4, NZ - 3, NZ - 2, NZ - 1):
        pl.semaphore_signal(barrier, inc=1, device_id=z_peer(k)[1], device_id_type=MESH)
    for k in range(1, NDP):
        pl.semaphore_signal(barrier, inc=1, device_id=dp_peer(k)[1], device_id_type=MESH)
    for k in range(1, NY):
        pl.semaphore_signal(barrier, inc=1, device_id=y_peer(k)[1], device_id_type=MESH)
        pl.semaphore_signal(barrier, inc=1, device_id={**y_peer(k)[1], **mate}, device_id_type=MESH)

    to_mate = remote(wo.at[1, own_head], wo.at[1, own_head], m_sem.at[0], m_sem.at[1], mate)

    loads = [pltpu.make_async_copy(tok_hbm, hid.at[0], load_sem.at[0])]
    for l in range(2):
        for p, w in enumerate((wr, wk, wv, wd, wa, wg)):
            loads.append(
                pltpu.make_async_copy(w.at[l], wt.at[l, pl.ds(64 * p, 64)], load_sem.at[1 + 6 * l + p])
            )
    state_loads = [pltpu.make_async_copy(st_hbm.at[l], st.at[l], load_sem.at[13 + l]) for l in range(2)]
    wo_loads = [pltpu.make_async_copy(wo_hbm.at[l], wo.at[l, own_head], load_sem.at[15 + 5 * l]) for l in range(2)]
    smalls = [
        pltpu.make_async_copy(a, b, load_sem.at[16 + i])
        for i, (a, b) in enumerate(
            ((gain_hbm, gain_ref), (floor_hbm, floor_ref), (direct_hbm, direct_ref), (norm_hbm, norm_ref))
        )
    ]
    loads[0].start()
    for cp in smalls:
        cp.start()
    for cp in loads[1:7]:
        cp.start()
    state_loads[0].start()
    wo_loads[0].start()
    for cp in loads[7:]:
        cp.start()
    state_loads[1].start()
    wo_loads[1].start()

    for l in range(2):
        if l == 0:
            loads[0].wait()
            for cp in smalls:
                cp.wait()
        for cp in loads[1 + 6 * l : 7 + 6 * l]:
            cp.wait()
        hv = hid[l].astype(F32).reshape(NZ, 4, 8, 128)
        sq = None
        xs = []
        for cg in range(4):
            part = hv[:, cg].reshape(256, 128)
            sq = part * part if sq is None else sq + part * part
            xs.append((part * gain_ref[l : l + 1, 128 * cg : 128 * cg + 128]).astype(BF16))
        high = sq.astype(BF16)
        ones = jnp.ones((8, 128), BF16)
        sums = lax.dot_general(ones, high, NT, preferred_element_type=F32) + lax.dot_general(
            ones, (sq - high.astype(F32)).astype(BF16), NT, preferred_element_type=F32
        )
        high = sums.astype(BF16).astype(F32)
        sums = jnp.where(lax.broadcasted_iota(jnp.int32, (8, 256), 0) == 0, high, sums - high).astype(BF16)
        tsend[l, 0] = sums[:, 0:128]
        tsend[l, 1] = sums[:, 128:256]
        proj = lax.dot_general(
            jnp.concatenate(xs, axis=1), wt[l], NT, preferred_element_type=F32
        ).astype(BF16)
        psend[l] = proj.reshape(NDP, SEQ, 384)
        if l == 0:
            with jax.named_scope("w_bar"):
                pl.semaphore_wait(barrier, 8 + (NDP - 1) + 2 * (NY - 1))
            wo_loads[0].wait()
            wo_gather()
            for k in (4, NZ - 4):
                pl.semaphore_signal(within8, inc=1, device_id=z_peer(k)[1], device_id_type=MESH)
        for k in (4, 3, 5, 2, 6, 1, 7):
            d, dev = dp_peer(k)
            remote(tsend.at[l, lax.div(d, 4)], trecv.at[l, di], t_ss.at[l], t_rs.at[l], dev).start()
        for k in (4, 3, 5, 2, 6, 1, 7):
            d, dev = dp_peer(k)
            remote(psend.at[l, d], precv.at[l, di], p_ss.at[l], p_rs.at[l], dev).start()
        if l == 0:
            wo_loads[1].wait()
            to_mate.start()
        with jax.named_scope("w_st"):
            state_loads[l].wait()
        stb[...] = st[l].reshape(SEQ * HC, HC).astype(BF16)
        if l == 0:
            with jax.named_scope("w_8"):
                pl.semaphore_wait(within8, 2)
            for k in (8, NZ - 8):
                pl.semaphore_signal(within16, inc=1, device_id=z_peer(k)[1], device_id_type=MESH)
        total = psend[l, di].astype(F32)
        with jax.named_scope("w_p"):
            remote(
                psend.at[l, pl.ds(0, NDP - 1)], precv.at[l, pl.ds(0, NDP - 1)], p_ss.at[l], p_rs.at[l], {"y": lax.rem(yi + 1, NY)}
            ).wait_recv()
        for k in range(1, NDP):
            total = total + precv[l, lax.rem(di + k, NDP)].astype(F32)
        some = trecv.at[l, pl.ds(0, NDP - 1)]
        remote(some, some, t_ss.at[l], t_rs.at[l], y_peer(1)[1]).wait_recv()
        squares = tsend[l, lax.div(di, 4)].astype(F32)
        for k in range(1, NDP):
            squares = squares + trecv[l, lax.rem(di + k, NDP)].astype(F32)
        squares = squares[0:1] + squares[1:2]
        picked = lax.broadcasted_iota(jnp.int32, (SEQ, 128), 1) == (
            lax.broadcasted_iota(jnp.int32, (SEQ, 128), 0) + SEQ * lax.rem(di, 4)
        )
        squares = jnp.sum(jnp.where(picked, squares, 0.0), axis=1, keepdims=True)
        total = total * lax.rsqrt(squares * (1.0 / D) + 1e-6)
        r, k_, v, pd, pa, pg = [total[:, 64 * p : 64 * p + 64] for p in range(6)]
        decay = jnp.exp(-0.6065306597126334 * jax.nn.sigmoid(floor_ref[l : l + 1, :] + pd))
        rate = jax.nn.sigmoid(pa)
        gate = jax.nn.sigmoid(pg)
        u = k_ * lax.rsqrt(jnp.sum(k_ * k_, axis=1, keepdims=True) + 1e-6)
        kr = k_ * rate
        ur = u * rate
        dr = decay * r
        row16 = lax.broadcasted_iota(jnp.int32, (16, 64), 0) % 8
        cs, ys = [], []
        for q in range(4):
            rows = slice(8 * q, 8 * q + 8)
            left = jnp.concatenate([u[rows], dr[rows]], axis=0).astype(BF16)
            res = lax.dot_general(left, stb[512 * q : 512 * q + 512], NT, preferred_element_type=F32)
            acc = jnp.zeros((16, 64), F32)
            for t in range(8):
                acc = jnp.where(row16 == t, res[:, 64 * t : 64 * t + 64], acc)
            cs.append(acc[0:8])
            ys.append(acc[8:16])
        c = -jnp.concatenate(cs, axis=0)
        y = (
            jnp.concatenate(ys, axis=0)
            + c * jnp.sum(ur * r, axis=1, keepdims=True)
            + v * jnp.sum(kr * r, axis=1, keepdims=True)
        )
        y = y - jnp.mean(y, axis=1, keepdims=True)
        var = jnp.mean(y * y, axis=1, keepdims=True)
        o = y * lax.rsqrt(var + 0.00064) * norm_ref[l : l + 1, :]
        o = o + jnp.sum(r * kr * direct_ref[l : l + 1, :], axis=1, keepdims=True) * v
        o = o * gate
        osend[l] = jnp.concatenate([o[0:16], o[16:32]], axis=1).astype(BF16)
        there = {"y": xi, "z": zi - odd + ci}
        for k in (4, 3, 5, 2, 6, 1, 7):
            remote(osend.at[l], oget.at[l, own_head], o_ss.at[l], o_rs.at[l], {**dp_peer(k)[1], **there}).start()

        @pl.when(jnp.logical_not(o_home))
        def _():
            remote(osend.at[l], oget.at[l, own_head], o_ss.at[l], o_rs.at[l], there).start()

        @pl.when(o_home)
        def _():
            oget[l, own_head] = osend[l]

        ct = c.T
        vt = v.T

        def update(lo, hi):
            for s in range(lo, hi):
                st_out[l, s] = (
                    st[l, s] * decay[s : s + 1, :]
                    + ct[:, s : s + 1] * ur[s : s + 1, :]
                    + vt[:, s : s + 1] * kr[s : s + 1, :]
                )

        with jax.named_scope("w_w"):
            some = wo.at[l, pl.ds(0, 7 - l)]
            remote(some, some, w_ss.at[l], w_rs.at[l], y_peer(1)[1]).wait_recv()
        with jax.named_scope("w_o"):
            o_count(l, lambda some: remote(some, some, o_ss.at[l], o_rs.at[l], y_peer(1)[1]).wait_recv())

        left = []
        for p in range(2 * NY):
            packed = oget[l, p]
            left.append(jnp.concatenate([packed[:, 0:64], packed[:, 64:128]], axis=0))
        share = lax.dot_general(
            jnp.concatenate(left, axis=1), wo[l].reshape(2 * NY * HC, 512), NN, preferred_element_type=F32
        ).astype(BF16)
        for n in range(16):
            rg, cg = n // 4, n % 4
            zsend[l, n % 8, n // 8] = share[8 * rg : 8 * rg + 8, 128 * cg : 128 * cg + 128]
        if l == 0:
            with jax.named_scope("w_16"):
                pl.semaphore_wait(within16, 2)

        def z_scatter(k, _):
            p, dev = z_peer(2 * far_first(k))
            src = zsend.at[l, lax.rem(lax.div(p, 2), 8)]
            remote(src, zrecv.at[l, place], z_ss.at[l], z_rs.at[l], dev).start()
            return 0

        with jax.named_scope("zsend"):
            lax.fori_loop(0, 15, z_scatter, 0)
        if l == 0:
            to_mate.wait_recv()
            for k in (2, 1, 3):
                for head in (own_head, mate_head):
                    remote(wo.at[1, head], wo.at[1, head], w_ss.at[1], w_rs.at[1], y_peer(k)[1]).start()
        zrecv[l, place] = zsend[l, lax.rem(place, 8)]
        with jax.named_scope("upd"):
            update(0, SEQ)
        with jax.named_scope("w_z"):
            some = zrecv.at[l, pl.ds(0, 15)]
            remote(some, some, z_ss.at[l], z_rs.at[l], z_peer(1)[1]).wait_recv()
        def pair(at):
            return hid.at[l + 1, yi, lax.rem(at, 2), :, lax.rem(lax.div(at, 2), 8)]

        mine = jnp.sum(zrecv[l].astype(F32), axis=0)
        for h in range(2):
            q = lax.rem(place, 8)
            hid[l + 1, yi, odd, h, q] = (mine[h] + hid[l, yi, odd, h, q].astype(F32)).astype(BF16)

        for g, (lo, hi) in enumerate(GROUPS):

            def z_gather(k, _):
                _, dev = z_peer(near_off(k))
                remote(pair(zi), pair(zi), g_ss.at[l], g_rs.at[l, g], dev).start()
                if g < DIRECT:
                    for i in (2, 1, 3):
                        both = {**dev, **y_peer(i)[1]}
                        remote(pair(zi), pair(zi), h_ss.at[l], h_rs.at[l], both).start()
                return 0

            with jax.named_scope("zsend"):
                lax.fori_loop(lo, hi, z_gather, 0)

        def forward(at):
            for k in (2, 1, 3):
                remote(pair(at), pair(at), h_ss.at[l], h_rs.at[l], y_peer(k)[1]).start()

        forward(zi)
        for g in range(len(GROUPS) - 1, -1, -1):
            lo, hi = GROUPS[g]
            with jax.named_scope("w_g"):
                some = zrecv.at[l, pl.ds(0, hi - lo)]
                remote(some, some, g_ss.at[l], g_rs.at[l, g], z_peer(1)[1]).wait_recv()

            def onward(k, _):
                forward(zi + NZ - near_off(k))
                return 0

            if g >= DIRECT:
                with jax.named_scope("fwd"):
                    lax.fori_loop(lo, hi, onward, 0)
        three = hid.at[l + 1, pl.ds(0, 3)]
        with jax.named_scope("w_h"):
            remote(three, three, h_ss.at[l], h_rs.at[l], {"y": lax.rem(yi + 1, NY)}).wait_recv()

    hid_out[...] = hid[2]
    to_mate.wait_send()
    for l in range(2):
        near = {"y": lax.rem(yi + 1, NY)}
        for buf, ss in (
            (trecv.at[l, pl.ds(0, NDP - 1)], t_ss),
            (psend.at[l, pl.ds(0, NDP - 1)], p_ss),
            (wo.at[l, pl.ds(0, 7 - l)], w_ss),
            (zrecv.at[l, pl.ds(0, 15)], z_ss),
            (zrecv.at[l, pl.ds(0, 15)], g_ss),
            (hid.at[l, pl.ds(0, 3)], h_ss),
        ):
            remote(buf, buf, ss.at[l], p_rs.at[l], near).wait_send()
        o_count(l, lambda some: remote(some, some, o_ss.at[l], o_rs.at[l], near).wait_send())


def finish(hid_ref, st_ref, hid_out, st_out, sem):
    copies = [pltpu.make_async_copy(hid_ref, hid_out, sem.at[8])]
    for i in range(8):
        part = (i // 4, pl.ds(8 * (i % 4), 8))
        copies.append(pltpu.make_async_copy(st_ref.at[part], st_out.at[part], sem.at[i]))
    for cp in copies:
        cp.start()
    for cp in copies:
        cp.wait()


def per_device(
    incoming_token, input_norm_gain, receptance_weight, key_weight, value_weight, decay_weight,
    learning_rate_weight, gate_weight, channel_decay_floor, direct_token_weight, head_norm_gain,
    output_weight, incoming_state,
):
    tiles = incoming_token.reshape(NZ, 8, 4, 128).transpose(0, 2, 1, 3).reshape(NY, 2, 2, 8, 8, 128)
    weights = [
        jnp.swapaxes(w, 1, 2)
        for w in (
            receptance_weight, key_weight, value_weight, decay_weight, learning_rate_weight, gate_weight,
        )
    ]
    state = incoming_state.reshape(2, SEQ, HC, HC)
    anywhere = pl.BlockSpec(memory_space=pl.ANY)
    vmem = pl.BlockSpec(memory_space=pltpu.VMEM)
    dma = pltpu.SemaphoreType.DMA
    hidden, new_state = pl.pallas_call(
        kernel,
        out_shape=(
            pltpu.VMEM((NY, 2, 2, 8, 8, 128), BF16),
            pltpu.VMEM((2, SEQ, HC, HC), F32),
        ),
        in_specs=[anywhere] * 13,
        out_specs=(vmem, vmem),
        scratch_shapes=[
            pltpu.VMEM((3, NY, 2, 2, 8, 8, 128), BF16),
            pltpu.VMEM((2, 512), F32),
            *[pltpu.VMEM((2, HC), F32) for _ in range(3)],
            pltpu.VMEM((2, 384, 512), BF16),
            pltpu.VMEM((2, 2 * NY, HC, 512), BF16),
            pltpu.VMEM((2, SEQ, HC, HC), F32),
            pltpu.VMEM((SEQ * HC, HC), BF16),
            pltpu.VMEM((2, 2, 8, 128), BF16),
            pltpu.VMEM((2, NDP, 8, 128), BF16),
            pltpu.VMEM((2, NDP, SEQ, 384), BF16),
            pltpu.VMEM((2, NDP, SEQ, 384), BF16),
            pltpu.VMEM((2, 16, 128), BF16),
            pltpu.VMEM((2, NY * NC, 16, 128), BF16),
            pltpu.VMEM((2, 8, 2, 8, 128), BF16),
            pltpu.VMEM((2, 16, 2, 8, 128), BF16),
            dma((21,)),
            *[dma((2,)) for _ in range(11)],
            dma((2, len(GROUPS))),
            *[dma((2,)) for _ in range(2)],
            dma((2,)),
            pltpu.SemaphoreType.REGULAR,
            pltpu.SemaphoreType.REGULAR,
        ],
        compiler_params=pltpu.CompilerParams(
            collective_id=0, has_side_effects=True, vmem_limit_bytes=60 * 1024 * 1024
        ),
        name="decode_step",
    )(
        tiles, input_norm_gain, *weights, channel_decay_floor, direct_token_weight, head_norm_gain,
        output_weight, state,
    )
    hidden, new_state = pl.pallas_call(
        finish,
        out_shape=(
            jax.ShapeDtypeStruct(hidden.shape, BF16),
            jax.ShapeDtypeStruct(new_state.shape, F32),
        ),
        in_specs=[vmem, vmem],
        out_specs=(anywhere, anywhere),
        scratch_shapes=[dma((9,))],
        compiler_params=pltpu.CompilerParams(vmem_limit_bytes=8 * 1024 * 1024),
        name="finish",
    )(hidden, new_state)
    hidden = hidden.reshape(NZ, 4, 8, 128).transpose(0, 2, 1, 3).reshape(256, 512)
    return (hidden, new_state.reshape(2, SEQ, 1, HC, HC))


def solution(mesh):
    finer = Mesh(mesh.devices.reshape(NZ, NY, NX, NC), ("z", "y", "x", "c"))
    tp, dp = ("z", "y"), ("x", "c")
    w = P(None, dp, tp)
    return jax.shard_map(
        per_device,
        mesh=finer,
        in_specs=(
            P(None, dp), P(None, dp), w, w, w, w, w, w, P(None, tp), P(None, tp), P(None, tp),
            P(None, tp, dp), P(None, dp, tp, None, None),
        ),
        out_specs=(P(None, dp), P(None, dp, tp, None, None)),
        check_vma=False,
    )
```
